512 devices in a mesh: sp: 64 (over z, y), fs: 4 (over x), tp: 2 (over core).
Axes of the slice: x: 4, y: 8, z: 8, core: 2. Of those that a mesh axis runs over, the one named last changes fastest.
Arguments:
- tokens: bfloat16 [4, 8192, 2048], P('fs', ('sp', 'tp')), may hold values from -6 to 6
- norm_gain: float32 [2048], replicated, may hold values from 0.1 to 1.9
- rec_query: bfloat16 [2048, 512], P('sp', 'tp'), may hold values from -0.125 to 0.125
- rec_input: bfloat16 [2048, 512], P('sp', 'tp'), may hold values from -0.125 to 0.125
- rec_forward: bfloat16 [2048, 512], P('sp', 'tp'), may hold values from -0.125 to 0.125
- rec_backward: bfloat16 [2048, 512], P('sp', 'tp'), may hold values from -0.125 to 0.125
- forget_gap: float32 [2, 512], P(None, 'tp'), may hold values from 0 to 0.06
- log_decay: float32 [4, 2, 4, 8192], P('fs', None, 'tp', 'sp'), may hold values from -0.7 to 0
- rec_gain: float32 [512], P('tp'), may hold values from 0.1 to 1.9
- conv_value: bfloat16 [2048, 512], P('sp', 'tp'), may hold values from -0.125 to 0.125
- conv_gate: bfloat16 [2048, 512], P('sp', 'tp'), may hold values from -0.125 to 0.125
- conv_kernel: bfloat16 [31, 512], P(None, 'tp'), may hold values from -3.1 to 3.1
- conv_gain: float32 [512], P('tp'), may hold values from 0.1 to 1.9
- out_rec: bfloat16 [512, 2048], P('tp', 'sp'), may hold values from -0.1875 to 0.1875
- out_conv: bfloat16 [512, 2048], P('tp', 'sp'), may hold values from -0.1875 to 0.1875
Outputs:
- mixed: bfloat16 [4, 8192, 2048], P('fs', ('sp', 'tp'))
The draws below stay inside these ranges and needn't reach their ends.
All inputs are finite; a program needn't handle non-finite values.
Results may differ from the reference program's by a relative error of at most 0.017.
Values may be sent and summed in bfloat16 or wider, within the bound.
No kernel may reach another device: no remote copies, remote signals or barrier semaphores. Data moves between devices by JAX's collectives and lax.ppermute only.
A program may use at most 64 MiB of HBM per device.

```python
import jax
import jax.numpy as jnp
from jax import lax

D = 2048
RECURRENCE_HEADS = 4
KD = 128
VD = 128
CONV_WIDTH = 31
BLOCK = 64
TOK_DEV = 128
SEQUENCE_LENGTH = 8192
SEQUENCE_COUNT = 4
GW = 512
KW = 512


def draw_forget_gap(key, part):
    rng_fast = jax.random.fold_in(key, 11)
    rng_gap = jax.random.fold_in(key, 12)
    fast_heads = jax.random.randint(rng_fast, (2, RECURRENCE_HEADS, 1), 0, 2) == 0
    spread = jax.random.uniform(rng_gap, (2, RECURRENCE_HEADS, KD), jnp.float32)
    fast_gap = 0.02 * jnp.power(3.0, spread)
    slow_gap = 0.2 * jnp.power(5.0, spread) / SEQUENCE_LENGTH
    chosen = jnp.where(fast_heads, fast_gap, slow_gap)
    return chosen.reshape(2, RECURRENCE_HEADS * KD).astype(jnp.float32)


def draw_log_decay(key, part):
    rng_rate = jax.random.fold_in(key, 21)
    random_spike_key = jax.random.fold_in(key, 22)
    random_length_key = jax.random.fold_in(key, 23)
    segments = SEQUENCE_LENGTH // TOK_DEV
    spread = jax.random.uniform(rng_rate, (SEQUENCE_COUNT, 2, RECURRENCE_HEADS, segments, 1), jnp.float32)
    spike_probability = 0.1 * jnp.power(10.0, spread) / SEQUENCE_LENGTH
    spike_probability = jnp.broadcast_to(spike_probability, (SEQUENCE_COUNT, 2, RECURRENCE_HEADS, segments, TOK_DEV)).reshape(SEQUENCE_COUNT, 2, RECURRENCE_HEADS, SEQUENCE_LENGTH)
    spike_active = jax.random.randint(random_spike_key, (SEQUENCE_COUNT, 2, RECURRENCE_HEADS, SEQUENCE_LENGTH), 0, SEQUENCE_LENGTH) < 2
    spike_length = jax.random.uniform(random_length_key, (SEQUENCE_COUNT, 2, RECURRENCE_HEADS, SEQUENCE_LENGTH), jnp.float32, 0.22, 0.69)
    return -(spike_probability + jnp.where(spike_active, spike_length, 0.0)).astype(jnp.float32)


def draw_conv_kernel(key, part):
    rng_base = jax.random.fold_in(key, 31)
    rng_scale = jax.random.fold_in(key, 32)
    channel_pos = jnp.arange(GW, dtype=jnp.float32) / max(GW - 1, 1)
    wobble = jax.random.uniform(rng_scale, (GW,), jnp.float32, jnp.log(0.7), jnp.log(1.4))
    channel_scale = jnp.exp(jnp.log(3.0) * channel_pos + wobble)
    base_draw = jnp.clip(jax.random.normal(rng_base, (CONV_WIDTH, GW), jnp.float32), -4.0, 4.0)
    return (base_draw * channel_scale[None, :] / jnp.sqrt(CONV_WIDTH * 1.0)).astype(jnp.bfloat16)


def block_levels(own_key, shape, split, least, largest):
    def one(dim, blocks):
        steps = jax.random.uniform(jax.random.fold_in(jax.random.fold_in(own_key, 6), dim), (blocks,), jnp.float32, least / len(split), largest / len(split))
        return jnp.repeat(jnp.exp(steps), shape[dim] // blocks).reshape((-1,) + (1,) * (len(shape) - dim - 1))

    gain = one(*split[0])
    for cut in split[1:]:
        gain = gain * one(*cut)
    return gain


def scatter_about(stream_key, dims, deviation, limit, cuts=(), kind=jnp.bfloat16):
    drawn = jax.random.normal(stream_key, dims, jnp.float32) * deviation
    if len(cuts) > 0:
        drawn = block_levels(stream_key, dims, cuts, -0.22, 0.18) * drawn
    return jnp.clip(drawn, min=-limit, max=limit).astype(kind)


def setup_inputs(seed: int = 0) -> dict:
    splits = jax.random.split(jax.random.key(seed), 16)
    return {
        "tokens": scatter_about(splits[0], (SEQUENCE_COUNT, SEQUENCE_LENGTH, D), 1.0, 6.0, ((0, 4), (1, 128))),
        "norm_gain": jnp.clip(1.0 + 0.18 * jax.random.normal(splits[1], (D,), jnp.float32), 0.1, 1.9),
        "rec_query": scatter_about(splits[2], (D, KW), D ** -0.5, 0.125, ((0, 64), (1, 2))),
        "rec_input": scatter_about(splits[3], (D, GW), D ** -0.5, 0.125, ((0, 64), (1, 2))),
        "rec_forward": scatter_about(splits[4], (D, KW), D ** -0.5, 0.125, ((0, 64), (1, 2))),
        "rec_backward": scatter_about(splits[5], (D, KW), D ** -0.5, 0.125, ((0, 64), (1, 2))),
        "forget_gap": draw_forget_gap(jax.random.fold_in(splits[15], 71), 0),
        "log_decay": draw_log_decay(jax.random.fold_in(splits[15], 71), 0),
        "rec_gain": jnp.clip(1.0 + 0.18 * jax.random.normal(splits[8], (GW,), jnp.float32), 0.1, 1.9),
        "conv_value": scatter_about(splits[9], (D, GW), D ** -0.5, 0.125, ((0, 64), (1, 2))),
        "conv_gate": scatter_about(splits[10], (D, GW), D ** -0.5, 0.125, ((0, 64), (1, 2))),
        "conv_kernel": draw_conv_kernel(jax.random.fold_in(splits[15], 71), 0),
        "conv_gain": jnp.clip(1.0 + 0.18 * jax.random.normal(splits[12], (GW,), jnp.float32), 0.1, 1.9),
        "out_rec": scatter_about(splits[13], (GW, D), (2 * GW) ** -0.5, 0.1875, ((0, 2), (1, 64))),
        "out_conv": scatter_about(splits[14], (GW, D), (2 * GW) ** -0.5, 0.1875, ((0, 2), (1, 64))),
    }


EPS = 1e-06
HIGH = lax.Precision.HIGHEST

def block_scan(queries, key_rows, value_rows, log_gate):
    heads_n, length_n, key_dim = queries.shape
    value_dim = value_rows.shape[-1]
    blocks = length_n // BLOCK

    def split_blocks(tensor):
        return tensor.reshape(heads_n, blocks, BLOCK, tensor.shape[-1]).transpose(1, 0, 2, 3)
    lower_mask = jnp.tril(jnp.ones((BLOCK, BLOCK), bool))

    def advance(states, inputs):
        query_b, key_b, value_b, gate_b = inputs
        cumulative = jnp.cumsum(gate_b, axis=1)
        query_g = query_b * jnp.exp(cumulative)
        key_g = key_b * jnp.exp(-cumulative)
        scores = jnp.einsum('htd,hsd->hts', query_g, key_g, precision=HIGH)
        scores = jnp.where(lower_mask, scores, 0.0)
        result = jnp.einsum('hts,hse->hte', scores, value_b, precision=HIGH)
        result = result + jnp.einsum('htd,hde->hte', query_g, states, precision=HIGH)
        last_g = cumulative[:, -1, :]
        weighted = key_b * jnp.exp(last_g[:, None, :] - cumulative)
        states = jnp.exp(last_g)[:, :, None] * states + jnp.einsum('hsd,hse->hde', weighted, value_b, precision=HIGH)
        return (states, result)
    start_state = jnp.zeros((heads_n, key_dim, value_dim), jnp.float32)
    inputs = (split_blocks(queries), split_blocks(key_rows), split_blocks(value_rows), split_blocks(log_gate))
    final_state, results = lax.scan(advance, start_state, inputs)
    return results.transpose(1, 0, 2, 3).reshape(heads_n, length_n, value_dim)

def to_heads(tensor):
    return tensor.astype(jnp.float32).reshape(tensor.shape[0], RECURRENCE_HEADS, -1).transpose(1, 0, 2)

def gate_terms(pre_act, gap_row, decay_row):
    closing = jax.nn.sigmoid(-to_heads(pre_act)) * gap_row.reshape(RECURRENCE_HEADS, 1, -1)
    return (closing, jnp.log1p(-closing) + decay_row[:, :, None])

def reference(tokens, norm_gain, rec_query, rec_input, rec_forward, rec_backward, forget_gap, log_decay, rec_gain, conv_value, conv_gate, conv_kernel, conv_gain, out_rec, out_conv):

    def one_sequence(inputs):
        rows_in, decay_in = inputs
        row_values = rows_in.astype(jnp.float32)
        normed = row_values * lax.rsqrt(lax.optimization_barrier(jnp.mean(row_values * row_values, axis=-1, keepdims=True)) + EPS)
        normed = (normed * norm_gain).astype(jnp.bfloat16)

        def project(weight):
            return jnp.dot(normed, weight, preferred_element_type=jnp.float32).astype(jnp.bfloat16)
        queries = jax.nn.silu(to_heads(project(rec_query))) * KD ** (-0.5)
        values = to_heads(project(rec_input))
        keys_fwd, gate_fwd = gate_terms(project(rec_forward), forget_gap[0], decay_in[0])
        keys_bwd, gate_bwd = gate_terms(project(rec_backward), forget_gap[1], decay_in[1])
        forward = block_scan(queries, keys_fwd, values, gate_fwd)
        backward = jnp.flip(block_scan(jnp.flip(queries, 1), jnp.flip(keys_bwd, 1), jnp.flip(values, 1), jnp.flip(gate_bwd, 1)), 1)
        joined = forward + backward
        joined = joined * lax.rsqrt(lax.optimization_barrier(jnp.mean(joined * joined, axis=-1, keepdims=True)) + EPS)
        joined = joined * rec_gain.reshape(RECURRENCE_HEADS, 1, VD)
        rec_out = joined.transpose(1, 0, 2).reshape(SEQUENCE_LENGTH, GW).astype(jnp.bfloat16)
        conv_pre = project(conv_value).astype(jnp.float32)
        glu_pre = project(conv_gate).astype(jnp.float32)
        gated = (conv_pre * jax.nn.sigmoid(glu_pre)).astype(jnp.bfloat16)
        convolved = lax.conv_general_dilated(gated.astype(jnp.float32)[None], conv_kernel.astype(jnp.float32)[:, None, :], (1,), 'SAME', dimension_numbers=('NWC', 'WIO', 'NWC'), feature_group_count=GW, precision=HIGH)[0]
        mean_c = lax.optimization_barrier(jnp.sum(convolved, axis=-1, keepdims=True)) / GW
        variance = lax.optimization_barrier(jnp.sum(convolved * convolved, axis=-1, keepdims=True)) / GW - mean_c * mean_c
        conv_out = jax.nn.silu((convolved - mean_c) * lax.rsqrt(variance + EPS) * conv_gain).astype(jnp.bfloat16)
        mixed = jnp.dot(rec_out, out_rec, preferred_element_type=jnp.float32)
        mixed = mixed + jnp.dot(conv_out, out_conv, preferred_element_type=jnp.float32)
        return mixed.astype(jnp.bfloat16)
    return lax.map(one_sequence, (tokens, log_decay))
```

```python
import functools

import jax
import jax.numpy as jnp
from jax import lax
from jax.experimental import pallas as pl
from jax.experimental.pallas import tpu as pltpu
from jax.sharding import Mesh
from jax.sharding import PartitionSpec as P

KD = 128
BLOCK = 64
EPS = 1e-06
Z, Y, X, C = "sp_0", "sp_1", "fs", "tp"
F32, BF16 = jnp.float32, jnp.bfloat16
NN = (((1,), (0,)), ((), ()))
NT = (((1,), (1,)), ((), ()))
TN = (((0,), (0,)), ((), ()))


def dot(a, b, dims):
    return lax.dot_general(a, b, dims, preferred_element_type=F32)


def sigmoid(x):
    return 1.0 / (1.0 + jnp.exp(-x))


def lanes(rows):
    return lax.broadcasted_iota(jnp.int32, (rows, 128), 1)


def triangles():
    r = lax.broadcasted_iota(jnp.int32, (128, 128), 0)
    c = lax.broadcasted_iota(jnp.int32, (128, 128), 1)
    same = (r // BLOCK) == (c // BLOCK)
    return same & (c <= r), same & (c >= r)


def split_dot(mask, x):
    hi = x.astype(BF16)
    lo = (x - hi.astype(F32)).astype(BF16)
    return dot(mask, hi, NN) + dot(mask, lo, NN)


def gate_keys(a, gap):
    return gap * sigmoid(-a)


def states_kernel(
    x_ref, w_ref, ld_ref, gap_ref,
    a_ref, v_ref, c_ref, gated_ref, send_ref, before_ref, offset_ref,
    chunk_s, chunk_t,
):
    step = pl.program_id(0)
    rows = x_ref.shape[0]
    acc = jnp.zeros((rows, 256), F32)
    acc_g = jnp.zeros((rows, 32), F32)
    for k in range(8):
        xk = x_ref[:, 256 * k : 256 * (k + 1)]
        acc += dot(xk, w_ref[k, :256, :], NN)
        acc_g += dot(xk, w_ref[k, 256:, :], NT)
    pre_a = acc[:, :128].astype(BF16)
    pre_v = acc[:, 128:].astype(BF16)
    a_ref[...] = pre_a
    v_ref[...] = pre_v
    glu = acc_g.astype(BF16).astype(F32)
    gated = pre_a.astype(F32)[:, 96:128] * sigmoid(glu)
    gated_ref[...] = gated.astype(BF16)
    lower, upper = triangles()
    lower_f, upper_f = lower.astype(F32), upper.astype(F32)
    lower_b, upper_b = lower_f.astype(BF16), upper_f.astype(BF16)
    lane = lanes(128)
    lane1 = lanes(1)
    for b in range(rows // 128):
        a = pre_a[128 * b : 128 * (b + 1)].astype(F32)
        v = pre_v[128 * b : 128 * (b + 1)]
        k = gate_keys(a, gap_ref[...])
        g = jnp.log1p(-k)
        ld = ld_ref[b]
        cum_f = split_dot(lower_b, g) + jnp.sum(lower_f * ld[0:1], axis=1, keepdims=True)
        cum_b = split_dot(upper_b, g) + jnp.sum(upper_f * ld[1:2], axis=1, keepdims=True)
        cum = jnp.where(lane < 32, cum_f, cum_b)
        c_ref[128 * b : 128 * (b + 1), :] = cum
        for h in range(2):
            part = slice(64 * h, 64 * (h + 1))
            cc = cum[part]
            tot = jnp.where(lane1 < 32, cc[63:64], cc[0:1])
            kd = (k[part] * jnp.exp(tot - cc)).astype(BF16)
            st = dot(v[part], kd, TN)
            packed = st[:64] + pltpu.roll(st[64:], 64, 1)
            tot8 = jnp.broadcast_to(tot, (8, 128))
            tot8 = jnp.where(lanes(8) < 64, tot8, pltpu.roll(tot8, 64, 1))
            idx = step * (rows // 64) + 2 * b + h
            chunk_s[idx] = packed
            chunk_t[idx] = tot8

    @pl.when(step == pl.num_programs(0) - 1)
    def _():
        n = chunk_s.shape[0]
        fwd = (lanes(64) % 64) < 32
        fwd8 = (lanes(8) % 64) < 32
        s = jnp.zeros((64, 128), F32)
        off = jnp.zeros((8, 128), F32)
        befores, offs = [None] * n, [None] * n
        for i in range(n):
            j = n - 1 - i
            befores[i], offs[i] = s, off
            tt = jnp.where(fwd8, chunk_t[i], chunk_t[j])
            sc = jnp.where(fwd, chunk_s[i], chunk_s[j])
            s = s * jnp.exp(tt)[0:1] + sc
            off = off + tt
        for i in range(n):
            j = n - 1 - i
            before_ref[i] = jnp.where(fwd, befores[i], befores[j]).astype(BF16)
            offset_ref[i] = jnp.where(fwd8, offs[i], offs[j])
        dec = jnp.exp(off)[0:1]
        hi = dec.astype(BF16)
        lo = (dec - hi.astype(F32)).astype(BF16)
        row = lax.broadcasted_iota(jnp.int32, (16, 128), 0)
        tail = jnp.where(row == 0, hi.astype(F32), jnp.where(row == 1, lo.astype(F32), 0.0))
        s = s.astype(BF16)
        tail = tail.astype(BF16)
        for i in range(8):
            send_ref[i, :64, :] = s
            send_ref[i, 64:, :] = tail


def local_kernel(a_ref, v_ref, c_ref, gap_ref, before_ref, offset_ref, out_ref, qd_ref):
    lower, upper = triangles()
    lane = lanes(128)
    for b in range(a_ref.shape[0] // 128):
        rows = slice(128 * b, 128 * (b + 1))
        a = a_ref[rows, :].astype(F32)
        v = v_ref[rows, :]
        cum = c_ref[rows, :]
        k = gate_keys(a, gap_ref[...])
        q = a * sigmoid(a) * (KD ** -0.5)
        q = jnp.where(lane < 32, pltpu.roll(q, 64, 1), pltpu.roll(q, 96, 1))
        q = jnp.where(lane < 64, q, 0.0)
        qg = q * jnp.exp(cum)
        kn = (k * jnp.exp(-cum)).astype(BF16)
        qf = jnp.where(lane < 32, qg, 0.0).astype(BF16)
        qb = jnp.where(lane < 32, 0.0, qg).astype(BF16)
        qh = qg.astype(BF16)
        scores = jnp.where(lower, dot(qf, kn, NT), 0.0) + jnp.where(upper, dot(qb, kn, NT), 0.0)
        out = dot(scores.astype(BF16), v, NN)
        for h in range(2):
            part = slice(64 * h, 64 * (h + 1))
            to = slice(128 * b + 64 * h, 128 * b + 64 * (h + 1))
            sb = before_ref[2 * b + h]
            full = jnp.concatenate([sb, pltpu.roll(sb.astype(F32), 64, 1).astype(BF16)], axis=0)
            out_ref[to, :] = out[part] + dot(qh[part], full, NT)
            qd_ref[to, :] = (qg[part] * jnp.exp(offset_ref[2 * b + h][0:1])).astype(BF16)


def conv_kernel_body(g_ref, left_ref, right_ref, w_ref, out_ref, pad):
    n = g_ref.shape[0]
    pad[0:16, :] = left_ref[...].astype(F32)
    pad[16 : 16 + n, :] = g_ref[...].astype(F32)
    pad[16 + n : 32 + n, :] = right_ref[...].astype(F32)
    w = w_ref[...]
    for blk in range(n // 64):
        acc = jnp.zeros((64, 32), F32)
        for j in range(31):
            acc += pad[64 * blk + j + 1 : 64 * blk + j + 65, :] * w[j : j + 1, :]
        out_ref[blk] = jnp.concatenate([acc[16 * q : 16 * (q + 1)] for q in range(4)], axis=1).astype(BF16)


def merge_kernel(z_ref, recv_ref, local_ref, qd_ref, conv_ref, send_ref):
    z = z_ref[0]
    fwd = (lanes(64) % 64) < 32
    fwd1 = (lanes(1) % 64) < 32
    s = jnp.zeros((64, 128), F32)
    for i in range(8):
        j = 7 - i
        sc = jnp.where(fwd, recv_ref[i, :64, :].astype(F32), recv_ref[j, :64, :].astype(F32))
        di = recv_ref[i, 64:80, :].astype(F32)
        dj = recv_ref[j, 64:80, :].astype(F32)
        dec = jnp.where(fwd1, di[0:1] + di[1:2], dj[0:1] + dj[1:2])
        pass_f = jnp.where(i < z, 1, 0)
        pass_b = jnp.where(j > z, 1, 0)
        passed = jnp.where(fwd, pass_f, pass_b) > 0
        s = jnp.where(passed, s * dec + sc, s)
    full = jnp.concatenate([s, pltpu.roll(s, 64, 1)], axis=0).astype(BF16)
    for blk in range(16):
        rows = slice(64 * blk, 64 * (blk + 1))
        out = local_ref[rows, :] + dot(qd_ref[rows, :], full, NT)
        send_ref[blk, :64, :] = out.astype(BF16)
        send_ref[blk, 64:, :] = conv_ref[blk]


def output_kernel(recv_ref, rec_gain_ref, conv_gain_ref, w_ref, out_ref, act):
    @pl.when(pl.program_id(0) == 0)
    def _():
        for c in range(2):
            for h in range(2):
                rec = sum(recv_ref[(4 * h + q) * 2 + c, :64, :].astype(F32) for q in range(4))
                rec = rec * lax.rsqrt(jnp.mean(rec * rec, axis=1, keepdims=True) + EPS)
                rec = rec * rec_gain_ref[2 * c + h : 2 * c + h + 1, :]
                at = 128 * (4 * c + h)
                act[:, at : at + 128] = rec.astype(BF16)
        lane = lanes(16) // 32
        blocks = []
        for c in range(2):
            for m in range(2):
                parts = [recv_ref[(4 * m + q) * 2 + c, 64:80, :].astype(F32) for q in range(4)]
                groups = []
                for g in range(4):
                    value = jnp.zeros((16, 128), F32)
                    for q in range(4):
                        moved = parts[q] if q == g else pltpu.roll(parts[q], (32 * (q - g)) % 128, 1)
                        value = jnp.where(lane == q, moved, value)
                    groups.append(value)
                blocks.append(jnp.concatenate(groups, axis=0))
        total = sum(jnp.sum(b, axis=1, keepdims=True) for b in blocks)
        square = sum(jnp.sum(b * b, axis=1, keepdims=True) for b in blocks)
        mean = total / 512.0
        scale = lax.rsqrt(square / 512.0 - mean * mean + EPS)
        for c in range(2):
            for m in range(2):
                n = 2 * c + m
                y = (blocks[n] - mean) * scale * conv_gain_ref[n : n + 1, :]
                at = 128 * (4 * c + 2 + m)
                act[:, at : at + 128] = (y * sigmoid(y)).astype(BF16)

    acc = jnp.zeros(out_ref.shape, F32)
    for b in range(8):
        acc += dot(act[:, 128 * b : 128 * (b + 1)], w_ref[b], NT)
    out_ref[...] = acc.astype(BF16)


def full(shape):
    return pl.BlockSpec(shape, lambda *_: (0,) * len(shape))


def spec(shape, at):
    return pl.BlockSpec(shape, at)


def body(
    tokens, norm_gain, rec_query, rec_input, rec_forward, rec_backward, forget_gap, log_decay,
    rec_gain, conv_value, conv_gate, conv_kernel, conv_gain, out_rec, out_conv,
):
    y, z, xi = lax.axis_index(Y), lax.axis_index(Z), lax.axis_index(X)

    rows_in = tokens[0].astype(F32)
    normed = rows_in * lax.rsqrt(jnp.mean(rows_in * rows_in, axis=-1, keepdims=True) + EPS)
    normed = (normed * norm_gain).astype(BF16)
    seq = lax.all_gather(normed, (Y, C), axis=0, tiled=True)

    def per_y(w):
        return w.reshape(32, 8, 32).transpose(1, 0, 2)

    values = jnp.repeat(rec_input.reshape(32, 2, 128).transpose(1, 0, 2), 4, axis=0)
    ld = jnp.repeat(log_decay[0].transpose(1, 0, 2), 4, axis=0)
    ld_hi = lax.reduce_precision(ld, 8, 7)
    ld_mid = lax.reduce_precision(ld - ld_hi, 8, 7)
    ld_lo = lax.reduce_precision(ld - ld_hi - ld_mid, 8, 7)
    ld3 = jnp.stack([ld_hi, ld_mid, ld_lo], axis=1).astype(BF16).reshape(8, 24, 32)
    ld3 = jnp.pad(ld3, ((0, 0), (0, 8), (0, 64)))
    outs = jnp.concatenate([out_rec, out_conv], axis=0).reshape(4, 128, 32)
    outs = lax.dynamic_index_in_dim(outs, xi, 0, keepdims=False).T
    first = jnp.concatenate(
        [
            per_y(rec_forward), per_y(rec_backward), per_y(rec_query), per_y(conv_value), values,
            per_y(conv_gate), ld3, jnp.broadcast_to(outs, (8, 32, 128)),
        ],
        axis=2,
    )
    first = lax.all_to_all(first, Y, split_axis=0, concat_axis=0, tiled=True)
    main = first[:, :, :256].reshape(256, 256)
    gate_t = first[:, :, 256:288].reshape(256, 32).T
    decays = first[:, :24, 288:320].astype(F32).reshape(8, 3, 2, 128).sum(axis=1)
    out_cols = first[:, :, 384:].reshape(256, 128)
    second = jnp.broadcast_to(jnp.concatenate([main, gate_t], axis=0), (8, 288, 256))
    weights = lax.all_to_all(second, Z, split_axis=0, concat_axis=0, tiled=True)
    out_w = lax.all_gather(out_cols, Z, axis=0, tiled=True)
    out_w = lax.all_gather(out_w, (C, X), axis=0)

    gains = lax.all_gather(jnp.stack([rec_gain, conv_gain]), C)
    rec_gains = gains[:, 0].reshape(4, 128)
    conv_gains = gains[:, 1].reshape(4, 128)
    gap = lax.dynamic_index_in_dim(forget_gap.reshape(2, 8, 32), y, 1, keepdims=False)
    gap = jnp.pad(gap.reshape(1, 64), ((0, 0), (0, 64)))
    taps = lax.dynamic_index_in_dim(conv_kernel.reshape(31, 8, 32), y, 1, keepdims=False)
    taps = jnp.pad(taps.astype(F32), ((0, 1), (0, 0)))

    n = seq.shape[0]
    tile = 256
    pre_a, pre_v, cum, gated, sent, before, offset = pl.pallas_call(
        states_kernel,
        grid=(n // tile,),
        in_specs=[
            spec((tile, 2048), lambda i: (i, 0)),
            full((8, 288, 256)),
            spec((tile // 128, 2, 128), lambda i: (i, 0, 0)),
            full((1, 128)),
        ],
        out_specs=[
            spec((tile, 128), lambda i: (i, 0)),
            spec((tile, 128), lambda i: (i, 0)),
            spec((tile, 128), lambda i: (i, 0)),
            spec((tile, 32), lambda i: (i, 0)),
            full((8, 80, 128)),
            full((16, 64, 128)),
            full((16, 8, 128)),
        ],
        out_shape=[
            jax.ShapeDtypeStruct((n, 128), BF16),
            jax.ShapeDtypeStruct((n, 128), BF16),
            jax.ShapeDtypeStruct((n, 128), F32),
            jax.ShapeDtypeStruct((n, 32), BF16),
            jax.ShapeDtypeStruct((8, 80, 128), BF16),
            jax.ShapeDtypeStruct((16, 64, 128), BF16),
            jax.ShapeDtypeStruct((16, 8, 128), F32),
        ],
        scratch_shapes=[pltpu.VMEM((16, 64, 128), F32), pltpu.VMEM((16, 8, 128), F32)],
        name="states",
    )(seq, weights, decays, gap)

    arrived = lax.all_to_all(sent, Z, split_axis=0, concat_axis=0, tiled=True)
    left = lax.ppermute(gated[n - 16 :], Z, [(i, i + 1) for i in range(7)])
    right = lax.ppermute(gated[:16], Z, [(i + 1, i) for i in range(7)])
    local, decayed = pl.pallas_call(
        local_kernel,
        out_shape=[jax.ShapeDtypeStruct((n, 128), F32), jax.ShapeDtypeStruct((n, 128), BF16)],
        name="local",
    )(pre_a, pre_v, cum, gap, before, offset)
    convolved = pl.pallas_call(
        conv_kernel_body,
        out_shape=jax.ShapeDtypeStruct((16, 16, 128), BF16),
        scratch_shapes=[pltpu.VMEM((n + 32, 32), F32)],
        name="conv",
    )(gated, left, right, taps)
    merged = pl.pallas_call(
        merge_kernel,
        in_specs=[pl.BlockSpec(memory_space=pltpu.SMEM)]
        + [pl.BlockSpec(memory_space=pltpu.VMEM)] * 4,
        out_shape=jax.ShapeDtypeStruct((16, 80, 128), BF16),
        name="merge",
    )(z.reshape(1).astype(jnp.int32), arrived, local, decayed, convolved)
    mine = lax.all_to_all(merged, (Y, C), split_axis=0, concat_axis=0, tiled=True)
    mixed = pl.pallas_call(
        output_kernel,
        grid=(4,),
        in_specs=[
            full((16, 80, 128)), full((4, 128)), full((4, 128)),
            spec((8, 512, 128), lambda i: (0, i, 0)),
        ],
        out_specs=spec((64, 512), lambda i: (0, i)),
        out_shape=jax.ShapeDtypeStruct((64, 2048), BF16),
        scratch_shapes=[pltpu.VMEM((64, 1024), BF16)],
        name="output",
    )(mine, rec_gains, conv_gains, out_w)
    return mixed[None]


def solution(mesh):
    finer = Mesh(
        mesh.devices.reshape(8, 8, mesh.shape["fs"], mesh.shape["tp"]), (Z, Y, X, C)
    )
    sp, sp_tp = (Z, Y), (Z, Y, C)
    row = P(sp, C)
    placed = (
        P(X, sp_tp, None), P(), row, row, row, row, P(None, C), P(X, None, C, sp), P(C),
        row, row, P(None, C), P(C), P(C, sp), P(C, sp),
    )
    return jax.shard_map(
        body, mesh=finer, in_specs=placed, out_specs=P(X, sp_tp, None), check_vma=False
    )
```

```python
import jax
import jax.numpy as jnp
from jax import lax
from jax.experimental import pallas as pl
from jax.experimental.pallas import tpu as pltpu
from jax.sharding import Mesh
from jax.sharding import PartitionSpec as P

KD = 128
BLOCK = 64
EPS = 1e-06
Z, Y, X, C = "sp_0", "sp_1", "fs", "tp"
F32, BF16 = jnp.float32, jnp.bfloat16
NN = (((1,), (0,)), ((), ()))
NT = (((1,), (1,)), ((), ()))
TN = (((0,), (0,)), ((), ()))


def dot(a, b, dims):
    return lax.dot_general(a, b, dims, preferred_element_type=F32)


def sigmoid(x):
    return 1.0 / (1.0 + jnp.exp(-x))


def lanes(rows):
    return lax.broadcasted_iota(jnp.int32, (rows, 128), 1)


def triangles():
    r = lax.broadcasted_iota(jnp.int32, (128, 128), 0)
    c = lax.broadcasted_iota(jnp.int32, (128, 128), 1)
    same = (r // BLOCK) == (c // BLOCK)
    return same & (c <= r), same & (c >= r)


def split_dot(mask, x):
    hi = x.astype(BF16)
    lo = (x - hi.astype(F32)).astype(BF16)
    return dot(mask, hi, NN) + dot(mask, lo, NN)


def gate_keys(a, gap):
    return gap * sigmoid(-a)


def norm_kernel(x_ref, gain_ref, out_ref):
    x = x_ref[...].astype(F32)
    scale = lax.rsqrt(jnp.mean(x * x, axis=1, keepdims=True) + EPS)
    out_ref[...] = (x * scale * gain_ref[...]).astype(BF16)


def first_kernel(
    x_ref, rf_ref, rb_ref, rq_ref, cv_ref, cg_ref, ri_ref, ld_ref, rec_ref, conv_ref, out_ref
):
    x = x_ref[0]
    lane = lanes(32)
    group = lane // 32
    row = lax.broadcasted_iota(jnp.int32, (32, 128), 0)
    at = pl.multiple_of(128 * (x % 2), 128)
    mine = jnp.where(x < 2, rec_ref[pl.ds(at, 128), :].astype(F32), conv_ref[pl.ds(at, 128), :].astype(F32))
    outs = mine.T.astype(BF16)
    for m in range(2):
        cols = slice(128 * m, 128 * (m + 1))
        src = [r[:, cols].astype(F32) for r in (rf_ref, rb_ref, rq_ref, cv_ref)]
        gate = cg_ref[:, cols].astype(F32)
        decays = jnp.zeros((32, 128), F32)
        for d in range(2):
            rest = jnp.broadcast_to(ld_ref[d, m : m + 1, :], (8, 128))
            for s in range(3):
                part = rest.astype(BF16).astype(F32)
                rest = rest - part
                low = pltpu.roll(part, 32, 1)[0:1]
                high = pltpu.roll(part, 64, 1)[0:1]
                decays = jnp.where(row == 2 * s + d, low, decays)
                decays = jnp.where(row == 6 + 2 * s + d, high, decays)
        for q in range(4):
            y = 4 * m + q
            a = jnp.zeros((32, 128), F32)
            for p in range(4):
                shift = (32 * (p - q)) % 128
                moved = pltpu.roll(src[p], shift, 1) if shift else src[p]
                a = jnp.where(group == p, moved, a)
            out_ref[y, :, 0:128] = a.astype(BF16)
            out_ref[y, :, 128:256] = ri_ref[:, cols]
            shift = (-32 * q) % 128
            moved = pltpu.roll(gate, shift, 1) if shift else gate
            out_ref[y, :, 256:384] = jnp.where(group == 0, moved, decays).astype(BF16)
            out_ref[y, :, 384:512] = outs


def second_kernel(first_ref, out_ref, cols_ref, ld_ref):
    lane = lanes(8)
    gates = []
    for y in range(8):
        third = first_ref[y, :, 256:384].astype(F32)
        gates.append(third)
        cols_ref[32 * y : 32 * (y + 1), :] = first_ref[y, :, 384:512]
        low = third[0:2] + third[2:4] + third[4:6]
        high = third[6:8] + third[8:10] + third[10:12]
        low = jnp.concatenate([low, low, low, low], axis=0)
        high = jnp.concatenate([high, high, high, high], axis=0)
        ld_ref[y] = jnp.where(lane < 96, pltpu.roll(low, 96, 1), pltpu.roll(high, 64, 1))[0:2]
    gate_t = jnp.concatenate(gates, axis=0).T[0:32].astype(BF16)
    for i in range(8):
        for y in range(8):
            out_ref[i, 32 * y : 32 * (y + 1), :] = first_ref[y, :, 0:256]
        out_ref[i, 256:288, :] = gate_t


def states_kernel(
    x_ref, w_ref, ld_ref, gap_ref,
    a_ref, v_ref, c_ref, gated_ref, send_ref, before_ref, offset_ref,
    chunk_s, chunk_t, edge,
):
    step = pl.program_id(0)
    rows = x_ref.shape[0]
    acc = jnp.zeros((rows, 256), F32)
    acc_g = jnp.zeros((rows, 32), F32)
    for k in range(8):
        xk = x_ref[:, 256 * k : 256 * (k + 1)]
        acc += dot(xk, w_ref[k, :256, :], NN)
        acc_g += dot(xk, w_ref[k, 256:, :], NT)
    pre_a = acc[:, :128].astype(BF16)
    pre_v = acc[:, 128:].astype(BF16)
    a_ref[...] = pre_a
    v_ref[...] = pre_v
    glu = acc_g.astype(BF16).astype(F32)
    gated = pre_a.astype(F32)[:, 96:128] * sigmoid(glu)
    gated_ref[...] = gated.astype(BF16)

    @pl.when(step == 0)
    def _():
        edge[...] = jnp.concatenate([gated[:16], gated[:16], gated[:16], gated[:16]], axis=1)

    @pl.when(step == pl.num_programs(0) - 1)
    def _():
        last = gated[rows - 16 :]
        last = jnp.concatenate([last, last, last, last], axis=1)
        edge[...] = jnp.where(lanes(16) < 32, edge[...], last)

    lower, upper = triangles()
    lower_f, upper_f = lower.astype(F32), upper.astype(F32)
    lower_b, upper_b = lower_f.astype(BF16), upper_f.astype(BF16)
    lane = lanes(128)
    lane1 = lanes(1)
    for b in range(rows // 128):
        a = pre_a[128 * b : 128 * (b + 1)].astype(F32)
        v = pre_v[128 * b : 128 * (b + 1)]
        k = gate_keys(a, gap_ref[...])
        g = jnp.log1p(-k)
        ld = ld_ref[b]
        cum_f = split_dot(lower_b, g) + jnp.sum(lower_f * ld[0:1], axis=1, keepdims=True)
        cum_b = split_dot(upper_b, g) + jnp.sum(upper_f * ld[1:2], axis=1, keepdims=True)
        cum = jnp.where(lane < 32, cum_f, cum_b)
        c_ref[128 * b : 128 * (b + 1), :] = cum
        for h in range(2):
            part = slice(64 * h, 64 * (h + 1))
            cc = cum[part]
            tot = jnp.where(lane1 < 32, cc[63:64], cc[0:1])
            kd = (k[part] * jnp.exp(tot - cc)).astype(BF16)
            st = dot(v[part], kd, TN)
            packed = st[:64] + pltpu.roll(st[64:], 64, 1)
            tot8 = jnp.broadcast_to(tot, (8, 128))
            tot8 = jnp.where(lanes(8) < 64, tot8, pltpu.roll(tot8, 64, 1))
            idx = step * (rows // 64) + 2 * b + h
            chunk_s[idx] = packed
            chunk_t[idx] = tot8

    @pl.when(step == pl.num_programs(0) - 1)
    def _():
        n = chunk_s.shape[0]
        fwd = (lanes(64) % 64) < 32
        fwd8 = (lanes(8) % 64) < 32
        s = jnp.zeros((64, 128), F32)
        off = jnp.zeros((8, 128), F32)
        befores, offs = [None] * n, [None] * n
        for i in range(n):
            j = n - 1 - i
            befores[i], offs[i] = s, off
            tt = jnp.where(fwd8, chunk_t[i], chunk_t[j])
            sc = jnp.where(fwd, chunk_s[i], chunk_s[j])
            s = s * jnp.exp(tt)[0:1] + sc
            off = off + tt
        for i in range(n):
            j = n - 1 - i
            before_ref[i] = jnp.where(fwd, befores[i], befores[j]).astype(BF16)
            offset_ref[i] = jnp.where(fwd8, offs[i], offs[j])
        dec = jnp.exp(off)[0:1]
        hi = dec.astype(BF16)
        lo = (dec - hi.astype(F32)).astype(BF16)
        row = lax.broadcasted_iota(jnp.int32, (16, 128), 0)
        tail = jnp.where(row == 0, hi.astype(F32), jnp.where(row == 1, lo.astype(F32), 0.0))
        s = s.astype(BF16)
        tail = tail.astype(BF16)
        for i in range(8):
            send_ref[i, :64, :] = s
            send_ref[i, 64:80, :] = tail
            send_ref[i, 80:96, :] = edge[...].astype(BF16)


def local_kernel(
    a_ref, v_ref, c_ref, gap_ref, before_ref, offset_ref, g_ref, taps_ref,
    out_ref, qd_ref, conv_ref, edge_ref, pad,
):
    n = g_ref.shape[0]
    zeros = jnp.zeros((16, 32), F32)
    pad[0:16, :] = zeros
    pad[16 : 16 + n, :] = g_ref[...].astype(F32)
    pad[16 + n : 32 + n, :] = zeros
    taps = taps_ref[...]
    for blk in range(n // 64):
        acc = jnp.zeros((64, 32), F32)
        for j in range(31):
            acc += pad[64 * blk + j + 1 : 64 * blk + j + 65, :] * taps[j : j + 1, :]
        conv_ref[blk] = jnp.concatenate([acc[16 * q : 16 * (q + 1)] for q in range(4)], axis=1).astype(BF16)
        if blk == 0:
            edge_ref[0] = acc[0:16]
        if blk == n // 64 - 1:
            edge_ref[1] = acc[48:64]
    lower, upper = triangles()
    lane = lanes(128)
    for b in range(a_ref.shape[0] // 128):
        rows = slice(128 * b, 128 * (b + 1))
        a = a_ref[rows, :].astype(F32)
        v = v_ref[rows, :]
        cum = c_ref[rows, :]
        k = gate_keys(a, gap_ref[...])
        q = a * sigmoid(a) * (KD ** -0.5)
        q = jnp.where(lane < 32, pltpu.roll(q, 64, 1), pltpu.roll(q, 96, 1))
        q = jnp.where(lane < 64, q, 0.0)
        qg = q * jnp.exp(cum)
        kn = (k * jnp.exp(-cum)).astype(BF16)
        qf = jnp.where(lane < 32, qg, 0.0).astype(BF16)
        qb = jnp.where(lane < 32, 0.0, qg).astype(BF16)
        qh = qg.astype(BF16)
        scores = jnp.where(lower, dot(qf, kn, NT), 0.0) + jnp.where(upper, dot(qb, kn, NT), 0.0)
        out = dot(scores.astype(BF16), v, NN)
        for h in range(2):
            part = slice(64 * h, 64 * (h + 1))
            to = slice(128 * b + 64 * h, 128 * b + 64 * (h + 1))
            sb = before_ref[2 * b + h]
            full = jnp.concatenate([sb, pltpu.roll(sb.astype(F32), 64, 1).astype(BF16)], axis=0)
            out_ref[to, :] = out[part] + dot(qh[part], full, NT)
            qd_ref[to, :] = (qg[part] * jnp.exp(offset_ref[2 * b + h][0:1])).astype(BF16)


def merge_kernel(z_ref, recv_ref, local_ref, qd_ref, conv_ref, edge_ref, taps_ref, send_ref):
    z = z_ref[0]
    heads = jnp.zeros((16, 128), F32)
    tails = jnp.zeros((16, 128), F32)
    for i in range(8):
        other = recv_ref[i, 80:96, :].astype(F32)
        tails = jnp.where(i == z - 1, other, tails)
        heads = jnp.where(i == z + 1, other, heads)
    zeros = jnp.zeros((16, 32), F32)
    before = jnp.concatenate([tails[:, 32:64], zeros], axis=0)
    after = jnp.concatenate([zeros, heads[:, 0:32]], axis=0)
    first, last = edge_ref[0], edge_ref[1]
    taps = taps_ref[...]
    for j in range(15):
        first += before[j + 1 : j + 17] * taps[j : j + 1, :]
        last += after[j + 1 : j + 17] * taps[16 + j : 17 + j, :]
    first = jnp.concatenate([first] * 4, axis=1).astype(BF16)
    last = jnp.concatenate([last] * 4, axis=1).astype(BF16)
    lane16 = lanes(16)
    fwd = (lanes(64) % 64) < 32
    fwd1 = (lanes(1) % 64) < 32
    s = jnp.zeros((64, 128), F32)
    for i in range(8):
        j = 7 - i
        sc = jnp.where(fwd, recv_ref[i, :64, :].astype(F32), recv_ref[j, :64, :].astype(F32))
        di = recv_ref[i, 64:80, :].astype(F32)
        dj = recv_ref[j, 64:80, :].astype(F32)
        dec = jnp.where(fwd1, di[0:1] + di[1:2], dj[0:1] + dj[1:2])
        pass_f = jnp.where(i < z, 1, 0)
        pass_b = jnp.where(j > z, 1, 0)
        passed = jnp.where(fwd, pass_f, pass_b) > 0
        s = jnp.where(passed, s * dec + sc, s)
    full = jnp.concatenate([s, pltpu.roll(s, 64, 1)], axis=0).astype(BF16)
    for blk in range(16):
        rows = slice(64 * blk, 64 * (blk + 1))
        out = local_ref[rows, :] + dot(qd_ref[rows, :], full, NT)
        send_ref[blk, :64, :] = out.astype(BF16)
        packed = conv_ref[blk]
        if blk == 0:
            packed = jnp.where(lane16 < 32, first, packed)
        if blk == 15:
            packed = jnp.where(lane16 >= 96, last, packed)
        send_ref[blk, 64:, :] = packed


def output_kernel(recv_ref, rec_gain_ref, conv_gain_ref, w_ref, out_ref, act):
    @pl.when(pl.program_id(0) == 0)
    def _():
        for c in range(2):
            for h in range(2):
                rec = sum(recv_ref[(4 * h + q) * 2 + c, :64, :].astype(F32) for q in range(4))
                rec = rec * lax.rsqrt(jnp.mean(rec * rec, axis=1, keepdims=True) + EPS)
                rec = rec * rec_gain_ref[2 * c + h : 2 * c + h + 1, :]
                at = 128 * (4 * c + h)
                act[:, at : at + 128] = rec.astype(BF16)
        lane = lanes(16) // 32
        blocks = []
        for c in range(2):
            for m in range(2):
                parts = [recv_ref[(4 * m + q) * 2 + c, 64:80, :].astype(F32) for q in range(4)]
                groups = []
                for g in range(4):
                    value = jnp.zeros((16, 128), F32)
                    for q in range(4):
                        moved = parts[q] if q == g else pltpu.roll(parts[q], (32 * (q - g)) % 128, 1)
                        value = jnp.where(lane == q, moved, value)
                    groups.append(value)
                blocks.append(jnp.concatenate(groups, axis=0))
        total = sum(jnp.sum(b, axis=1, keepdims=True) for b in blocks)
        square = sum(jnp.sum(b * b, axis=1, keepdims=True) for b in blocks)
        mean = total / 512.0
        scale = lax.rsqrt(square / 512.0 - mean * mean + EPS)
        for c in range(2):
            for m in range(2):
                n = 2 * c + m
                y = (blocks[n] - mean) * scale * conv_gain_ref[n : n + 1, :]
                at = 128 * (4 * c + 2 + m)
                act[:, at : at + 128] = (y * sigmoid(y)).astype(BF16)

    acc = jnp.zeros(out_ref.shape, F32)
    for b in range(8):
        acc += dot(act[:, 128 * b : 128 * (b + 1)], w_ref[b], NT)
    out_ref[...] = acc.astype(BF16)


def full(shape):
    return pl.BlockSpec(shape, lambda *_: (0,) * len(shape))


def spec(shape, at):
    return pl.BlockSpec(shape, at)


def body(
    tokens, norm_gain, rec_query, rec_input, rec_forward, rec_backward, forget_gap, log_decay,
    rec_gain, conv_value, conv_gate, conv_kernel, conv_gain, out_rec, out_conv,
):
    y, z, xi = lax.axis_index(Y), lax.axis_index(Z), lax.axis_index(X)

    normed = pl.pallas_call(
        norm_kernel, out_shape=jax.ShapeDtypeStruct((64, 2048), BF16), name="norm"
    )(tokens[0], norm_gain.reshape(1, 2048))
    seq = lax.all_gather(normed, (Y, C), axis=0, tiled=True)

    first = pl.pallas_call(
        first_kernel,
        in_specs=[pl.BlockSpec(memory_space=pltpu.SMEM)]
        + [pl.BlockSpec(memory_space=pltpu.VMEM)] * 9,
        out_shape=jax.ShapeDtypeStruct((8, 32, 512), BF16),
        name="first",
    )(
        xi.reshape(1).astype(jnp.int32), rec_forward, rec_backward, rec_query, conv_value,
        conv_gate, rec_input, log_decay[0], out_rec, out_conv,
    )
    first = lax.all_to_all(first, Y, split_axis=0, concat_axis=0, tiled=True)
    second, out_cols, decays = pl.pallas_call(
        second_kernel,
        out_shape=[
            jax.ShapeDtypeStruct((8, 288, 256), BF16),
            jax.ShapeDtypeStruct((256, 128), BF16),
            jax.ShapeDtypeStruct((8, 2, 128), F32),
        ],
        name="second",
    )(first)
    weights = lax.all_to_all(second, Z, split_axis=0, concat_axis=0, tiled=True)
    out_w = lax.all_gather(out_cols, Z, axis=0, tiled=True)
    out_w = lax.all_gather(out_w, (C, X), axis=0)

    gains = lax.all_gather(jnp.stack([rec_gain, conv_gain]), C)
    rec_gains = gains[:, 0].reshape(4, 128)
    conv_gains = gains[:, 1].reshape(4, 128)
    gap = lax.dynamic_index_in_dim(forget_gap.reshape(2, 8, 32), y, 1, keepdims=False)
    gap = jnp.pad(gap.reshape(1, 64), ((0, 0), (0, 64)))
    taps = lax.dynamic_index_in_dim(conv_kernel.reshape(31, 8, 32), y, 1, keepdims=False)
    taps = jnp.pad(taps.astype(F32), ((0, 1), (0, 0)))

    n = seq.shape[0]
    tile = 256
    pre_a, pre_v, cum, gated, sent, before, offset = pl.pallas_call(
        states_kernel,
        grid=(n // tile,),
        in_specs=[
            spec((tile, 2048), lambda i: (i, 0)),
            full((8, 288, 256)),
            spec((tile // 128, 2, 128), lambda i: (i, 0, 0)),
            full((1, 128)),
        ],
        out_specs=[
            spec((tile, 128), lambda i: (i, 0)),
            spec((tile, 128), lambda i: (i, 0)),
            spec((tile, 128), lambda i: (i, 0)),
            spec((tile, 32), lambda i: (i, 0)),
            full((8, 96, 128)),
            full((16, 64, 128)),
            full((16, 8, 128)),
        ],
        out_shape=[
            jax.ShapeDtypeStruct((n, 128), BF16),
            jax.ShapeDtypeStruct((n, 128), BF16),
            jax.ShapeDtypeStruct((n, 128), F32),
            jax.ShapeDtypeStruct((n, 32), BF16),
            jax.ShapeDtypeStruct((8, 96, 128), BF16),
            jax.ShapeDtypeStruct((16, 64, 128), BF16),
            jax.ShapeDtypeStruct((16, 8, 128), F32),
        ],
        scratch_shapes=[
            pltpu.VMEM((16, 64, 128), F32), pltpu.VMEM((16, 8, 128), F32), pltpu.VMEM((16, 128), F32)
        ],
        name="states",
    )(seq, weights, decays, gap)

    arrived = lax.all_to_all(sent, Z, split_axis=0, concat_axis=0, tiled=True)
    local, decayed, convolved, edges = pl.pallas_call(
        local_kernel,
        out_shape=[
            jax.ShapeDtypeStruct((n, 128), F32),
            jax.ShapeDtypeStruct((n, 128), BF16),
            jax.ShapeDtypeStruct((16, 16, 128), BF16),
            jax.ShapeDtypeStruct((2, 16, 32), F32),
        ],
        scratch_shapes=[pltpu.VMEM((n + 32, 32), F32)],
        name="local",
    )(pre_a, pre_v, cum, gap, before, offset, gated, taps)
    merged = pl.pallas_call(
        merge_kernel,
        in_specs=[pl.BlockSpec(memory_space=pltpu.SMEM)]
        + [pl.BlockSpec(memory_space=pltpu.VMEM)] * 6,
        out_shape=jax.ShapeDtypeStruct((16, 80, 128), BF16),
        name="merge",
    )(z.reshape(1).astype(jnp.int32), arrived, local, decayed, convolved, edges, taps)
    mine = lax.all_to_all(merged, (Y, C), split_axis=0, concat_axis=0, tiled=True)
    mixed = pl.pallas_call(
        output_kernel,
        grid=(4,),
        in_specs=[
            full((16, 80, 128)), full((4, 128)), full((4, 128)),
            spec((8, 512, 128), lambda i: (0, i, 0)),
        ],
        out_specs=spec((64, 512), lambda i: (0, i)),
        out_shape=jax.ShapeDtypeStruct((64, 2048), BF16),
        scratch_shapes=[pltpu.VMEM((64, 1024), BF16)],
        name="output",
    )(mine, rec_gains, conv_gains, out_w)
    return mixed[None]


def solution(mesh):
    finer = Mesh(
        mesh.devices.reshape(8, 8, mesh.shape["fs"], mesh.shape["tp"]), (Z, Y, X, C)
    )
    sp, sp_tp = (Z, Y), (Z, Y, C)
    row = P(sp, C)
    placed = (
        P(X, sp_tp, None), P(), row, row, row, row, P(None, C), P(X, None, C, sp), P(C),
        row, row, P(None, C), P(C), P(C, sp), P(C, sp),
    )
    return jax.shard_map(
        body, mesh=finer, in_specs=placed, out_specs=P(X, sp_tp, None), check_vma=False
    )
```

```python
import jax
import jax.numpy as jnp
from jax import lax
from jax.experimental import pallas as pl
from jax.experimental.pallas import tpu as pltpu
from jax.sharding import Mesh
from jax.sharding import PartitionSpec as P

KD = 128
BLOCK = 64
EPS = 1e-06
Z, Y, X, C = "sp_0", "sp_1", "fs", "tp"
F32, BF16 = jnp.float32, jnp.bfloat16
NN = (((1,), (0,)), ((), ()))
NT = (((1,), (1,)), ((), ()))
TN = (((0,), (0,)), ((), ()))


def dot(a, b, dims):
    return lax.dot_general(a, b, dims, preferred_element_type=F32)


def sigmoid(x):
    return 1.0 / (1.0 + jnp.exp(-x))


def lanes(rows):
    return lax.broadcasted_iota(jnp.int32, (rows, 128), 1)


def triangles():
    r = lax.broadcasted_iota(jnp.int32, (128, 128), 0)
    c = lax.broadcasted_iota(jnp.int32, (128, 128), 1)
    same = (r // BLOCK) == (c // BLOCK)
    return same & (c <= r), same & (c >= r)


def split_dot(mask, x):
    hi = x.astype(BF16)
    lo = (x - hi.astype(F32)).astype(BF16)
    return dot(mask, hi, NN) + dot(mask, lo, NN)


def gate_keys(a, gap):
    return gap * sigmoid(-a)


def norm_kernel(x_ref, gain_ref, out_ref):
    x = x_ref[...].astype(F32)
    scale = lax.rsqrt(jnp.mean(x * x, axis=1, keepdims=True) + EPS)
    out_ref[...] = (x * scale * gain_ref[...]).astype(BF16)


def first_kernel(
    rf_ref, rb_ref, rq_ref, cv_ref, cg_ref, ri_ref, ld_ref, rec_ref, conv_ref, out_ref
):
    group = lanes(32) // 32
    row = lax.broadcasted_iota(jnp.int32, (32, 128), 0)
    for m in range(2):
        cols = slice(128 * m, 128 * (m + 1))
        src = [r[:, cols].astype(F32) for r in (rf_ref, rb_ref, rq_ref, cv_ref)]
        gate = cg_ref[:, cols].astype(F32)
        decays = jnp.zeros((32, 128), F32)
        for d in range(2):
            rest = jnp.broadcast_to(ld_ref[d, m : m + 1, :], (8, 128))
            for s in range(3):
                part = rest.astype(BF16).astype(F32)
                rest = rest - part
                low = pltpu.roll(part, 32, 1)[0:1]
                high = pltpu.roll(part, 64, 1)[0:1]
                decays = jnp.where(row == 2 * s + d, low, decays)
                decays = jnp.where(row == 6 + 2 * s + d, high, decays)
        for q in range(4):
            y = 4 * m + q
            a = jnp.zeros((32, 128), F32)
            for p in range(4):
                shift = (32 * (p - q)) % 128
                moved = pltpu.roll(src[p], shift, 1) if shift else src[p]
                a = jnp.where(group == p, moved, a)
            out_ref[y, :, 0:128] = a.astype(BF16)
            out_ref[y, :, 128:256] = ri_ref[:, cols]
            shift = (-32 * q) % 128
            moved = pltpu.roll(gate, shift, 1) if shift else gate
            out_ref[y, :, 256:384] = jnp.where(group == 0, moved, decays).astype(BF16)
            out_ref[y, :, 384:640] = rec_ref[...]
            out_ref[y, :, 640:896] = conv_ref[...]


def second_kernel(first_ref, w_ref, w2_ref, cols_ref, ld_ref):
    lane = lanes(8)
    keys, values, gates = [], [], []
    for y in range(8):
        third = first_ref[y, :, 256:384].astype(F32)
        keys.append(first_ref[y, :, 0:128].astype(F32))
        values.append(first_ref[y, :, 128:256].astype(F32))
        gates.append(third)
        cols_ref[32 * y : 32 * (y + 1), :] = first_ref[y, :, 384:896]
        low = third[0:2] + third[2:4] + third[4:6]
        high = third[6:8] + third[8:10] + third[10:12]
        low = jnp.concatenate([low, low, low, low], axis=0)
        high = jnp.concatenate([high, high, high, high], axis=0)
        ld_ref[y] = jnp.where(lane < 96, pltpu.roll(low, 96, 1), pltpu.roll(high, 64, 1))[0:2]
    keys = jnp.concatenate(keys, axis=0).T.astype(BF16)
    w_ref[0:128, :] = jnp.concatenate(values, axis=0).T.astype(BF16)
    w_ref[128:224, :] = keys[0:96]
    gates = jnp.concatenate(gates, axis=0).T[0:32].astype(BF16)
    for i in range(8):
        w2_ref[i, 0:32, :] = keys[96:128]
        w2_ref[i, 32:64, :] = gates


def states_kernel(
    x_ref, w_ref, w2_ref, ld_ref, gap_ref,
    a_ref, v_ref, c_ref, gated_ref, send_ref, before_ref, offset_ref,
    chunk_s, chunk_t, edge,
):
    step = pl.program_id(0)
    rows = x_ref.shape[0]
    acc = jnp.zeros((rows, 224), F32)
    acc_g = jnp.zeros((rows, 64), F32)
    for k in range(8):
        xk = x_ref[:, 256 * k : 256 * (k + 1)]
        acc += dot(xk, w_ref[k], NT)
        acc_g += dot(xk, w2_ref[k], NT)
    pre_v = acc[:, :128].astype(BF16)
    pre_a = jnp.concatenate([acc[:, 128:], jnp.zeros((rows, 32), F32)], axis=1).astype(BF16)
    a_ref[...] = pre_a
    v_ref[...] = pre_v
    glu = acc_g.astype(BF16).astype(F32)
    gated = glu[:, 0:32] * sigmoid(glu[:, 32:64])
    gated_ref[...] = gated.astype(BF16)

    @pl.when(step == 0)
    def _():
        edge[...] = jnp.concatenate([gated[:16], gated[:16], gated[:16], gated[:16]], axis=1)

    @pl.when(step == pl.num_programs(0) - 1)
    def _():
        last = gated[rows - 16 :]
        last = jnp.concatenate([last, last, last, last], axis=1)
        edge[...] = jnp.where(lanes(16) < 32, edge[...], last)

    lower, upper = triangles()
    lower_f, upper_f = lower.astype(F32), upper.astype(F32)
    lower_b, upper_b = lower_f.astype(BF16), upper_f.astype(BF16)
    lane = lanes(128)
    lane1 = lanes(1)
    for b in range(rows // 128):
        a = pre_a[128 * b : 128 * (b + 1)].astype(F32)
        v = pre_v[128 * b : 128 * (b + 1)]
        k = gate_keys(a, gap_ref[...])
        g = jnp.log1p(-k)
        ld = ld_ref[b]
        cum_f = split_dot(lower_b, g) + jnp.sum(lower_f * ld[0:1], axis=1, keepdims=True)
        cum_b = split_dot(upper_b, g) + jnp.sum(upper_f * ld[1:2], axis=1, keepdims=True)
        cum = jnp.where(lane < 32, cum_f, cum_b)
        c_ref[128 * b : 128 * (b + 1), :] = cum
        for h in range(2):
            part = slice(64 * h, 64 * (h + 1))
            cc = cum[part]
            tot = jnp.where(lane1 < 32, cc[63:64], cc[0:1])
            kd = (k[part] * jnp.exp(tot - cc)).astype(BF16)
            st = dot(v[part], kd, TN)
            packed = st[:64] + pltpu.roll(st[64:], 64, 1)
            tot8 = jnp.broadcast_to(tot, (8, 128))
            tot8 = jnp.where(lanes(8) < 64, tot8, pltpu.roll(tot8, 64, 1))
            idx = step * (rows // 64) + 2 * b + h
            chunk_s[idx] = packed
            chunk_t[idx] = tot8

    @pl.when(step == pl.num_programs(0) - 1)
    def _():
        n = chunk_s.shape[0]
        fwd = (lanes(64) % 64) < 32
        fwd8 = (lanes(8) % 64) < 32
        s = jnp.zeros((64, 128), F32)
        off = jnp.zeros((8, 128), F32)
        befores, offs = [None] * n, [None] * n
        for i in range(n):
            j = n - 1 - i
            befores[i], offs[i] = s, off
            tt = jnp.where(fwd8, chunk_t[i], chunk_t[j])
            sc = jnp.where(fwd, chunk_s[i], chunk_s[j])
            s = s * jnp.exp(tt)[0:1] + sc
            off = off + tt
        for i in range(n):
            j = n - 1 - i
            before_ref[i] = jnp.where(fwd, befores[i], befores[j]).astype(BF16)
            offset_ref[i] = jnp.where(fwd8, offs[i], offs[j])
        dec = jnp.exp(off)[0:1]
        hi = dec.astype(BF16)
        lo = (dec - hi.astype(F32)).astype(BF16)
        row = lax.broadcasted_iota(jnp.int32, (16, 128), 0)
        tail = jnp.where(row == 0, hi.astype(F32), jnp.where(row == 1, lo.astype(F32), 0.0))
        s = s.astype(BF16)
        tail = tail.astype(BF16)
        for i in range(8):
            send_ref[i, :64, :] = s
            send_ref[i, 64:80, :] = tail
            send_ref[i, 80:96, :] = edge[...].astype(BF16)


def local_kernel(
    a_ref, v_ref, c_ref, gap_ref, before_ref, offset_ref, g_ref, taps_ref,
    out_ref, qd_ref, conv_ref, edge_ref, pad,
):
    n = g_ref.shape[0]
    zeros = jnp.zeros((16, 32), F32)
    pad[0:16, :] = zeros
    pad[16 : 16 + n, :] = g_ref[...].astype(F32)
    pad[16 + n : 32 + n, :] = zeros
    taps = taps_ref[...]
    for blk in range(n // 64):
        acc = jnp.zeros((64, 32), F32)
        for j in range(31):
            acc += pad[64 * blk + j + 1 : 64 * blk + j + 65, :] * taps[j : j + 1, :]
        conv_ref[blk] = jnp.concatenate([acc[16 * q : 16 * (q + 1)] for q in range(4)], axis=1).astype(BF16)
        if blk == 0:
            edge_ref[0] = acc[0:16]
        if blk == n // 64 - 1:
            edge_ref[1] = acc[48:64]
    lower, upper = triangles()
    lane = lanes(128)
    for b in range(a_ref.shape[0] // 128):
        rows = slice(128 * b, 128 * (b + 1))
        a = a_ref[rows, :].astype(F32)
        v = v_ref[rows, :]
        cum = c_ref[rows, :]
        k = gate_keys(a, gap_ref[...])
        q = a * sigmoid(a) * (KD ** -0.5)
        q = jnp.where(lane < 32, pltpu.roll(q, 64, 1), pltpu.roll(q, 96, 1))
        q = jnp.where(lane < 64, q, 0.0)
        qg = q * jnp.exp(cum)
        kn = (k * jnp.exp(-cum)).astype(BF16)
        qf = jnp.where(lane < 32, qg, 0.0).astype(BF16)
        qb = jnp.where(lane < 32, 0.0, qg).astype(BF16)
        qh = qg.astype(BF16)
        scores = jnp.where(lower, dot(qf, kn, NT), 0.0) + jnp.where(upper, dot(qb, kn, NT), 0.0)
        out = dot(scores.astype(BF16), v, NN)
        for h in range(2):
            part = slice(64 * h, 64 * (h + 1))
            to = slice(128 * b + 64 * h, 128 * b + 64 * (h + 1))
            sb = before_ref[2 * b + h]
            full = jnp.concatenate([sb, pltpu.roll(sb.astype(F32), 64, 1).astype(BF16)], axis=0)
            out_ref[to, :] = out[part] + dot(qh[part], full, NT)
            qd_ref[to, :] = (qg[part] * jnp.exp(offset_ref[2 * b + h][0:1])).astype(BF16)


def merge_kernel(z_ref, recv_ref, local_ref, qd_ref, conv_ref, edge_ref, taps_ref, send_ref):
    z = z_ref[0]
    heads = jnp.zeros((16, 128), F32)
    tails = jnp.zeros((16, 128), F32)
    for i in range(8):
        other = recv_ref[i, 80:96, :].astype(F32)
        tails = jnp.where(i == z - 1, other, tails)
        heads = jnp.where(i == z + 1, other, heads)
    zeros = jnp.zeros((16, 32), F32)
    before = jnp.concatenate([tails[:, 32:64], zeros], axis=0)
    after = jnp.concatenate([zeros, heads[:, 0:32]], axis=0)
    first, last = edge_ref[0], edge_ref[1]
    taps = taps_ref[...]
    for j in range(15):
        first += before[j + 1 : j + 17] * taps[j : j + 1, :]
        last += after[j + 1 : j + 17] * taps[16 + j : 17 + j, :]
    first = jnp.concatenate([first] * 4, axis=1).astype(BF16)
    last = jnp.concatenate([last] * 4, axis=1).astype(BF16)
    lane16 = lanes(16)
    fwd = (lanes(64) % 64) < 32
    fwd1 = (lanes(1) % 64) < 32
    s = jnp.zeros((64, 128), F32)
    for i in range(8):
        j = 7 - i
        sc = jnp.where(fwd, recv_ref[i, :64, :].astype(F32), recv_ref[j, :64, :].astype(F32))
        di = recv_ref[i, 64:80, :].astype(F32)
        dj = recv_ref[j, 64:80, :].astype(F32)
        dec = jnp.where(fwd1, di[0:1] + di[1:2], dj[0:1] + dj[1:2])
        pass_f = jnp.where(i < z, 1, 0)
        pass_b = jnp.where(j > z, 1, 0)
        passed = jnp.where(fwd, pass_f, pass_b) > 0
        s = jnp.where(passed, s * dec + sc, s)
    full = jnp.concatenate([s, pltpu.roll(s, 64, 1)], axis=0).astype(BF16)
    for blk in range(16):
        rows = slice(64 * blk, 64 * (blk + 1))
        out = local_ref[rows, :] + dot(qd_ref[rows, :], full, NT)
        send_ref[blk, :64, :] = out.astype(BF16)
        packed = conv_ref[blk]
        if blk == 0:
            packed = jnp.where(lane16 < 32, first, packed)
        if blk == 15:
            packed = jnp.where(lane16 >= 96, last, packed)
        send_ref[blk, 64:, :] = packed


def output_kernel(recv_ref, rec_gain_ref, conv_gain_ref, w_ref, out_ref, act):
    @pl.when(pl.program_id(0) == 0)
    def _():
        for c in range(2):
            for h in range(2):
                rec = sum(recv_ref[(4 * h + q) * 2 + c, :64, :].astype(F32) for q in range(4))
                rec = rec * lax.rsqrt(jnp.mean(rec * rec, axis=1, keepdims=True) + EPS)
                rec = rec * rec_gain_ref[2 * c + h : 2 * c + h + 1, :]
                at = 128 * (4 * c + h)
                act[:, at : at + 128] = rec.astype(BF16)
        lane = lanes(16) // 32
        blocks = []
        for c in range(2):
            for m in range(2):
                parts = [recv_ref[(4 * m + q) * 2 + c, 64:80, :].astype(F32) for q in range(4)]
                groups = []
                for g in range(4):
                    value = jnp.zeros((16, 128), F32)
                    for q in range(4):
                        moved = parts[q] if q == g else pltpu.roll(parts[q], (32 * (q - g)) % 128, 1)
                        value = jnp.where(lane == q, moved, value)
                    groups.append(value)
                blocks.append(jnp.concatenate(groups, axis=0))
        total = sum(jnp.sum(b, axis=1, keepdims=True) for b in blocks)
        square = sum(jnp.sum(b * b, axis=1, keepdims=True) for b in blocks)
        mean = total / 512.0
        scale = lax.rsqrt(square / 512.0 - mean * mean + EPS)
        for c in range(2):
            for m in range(2):
                n = 2 * c + m
                y = (blocks[n] - mean) * scale * conv_gain_ref[n : n + 1, :]
                at = 128 * (4 * c + 2 + m)
                act[:, at : at + 128] = (y * sigmoid(y)).astype(BF16)

    acc = jnp.zeros(out_ref.shape, F32)
    for c in range(2):
        acc += dot(act[:, 512 * c : 512 * (c + 1)], w_ref[c], NT)
    out_ref[...] = acc.astype(BF16)


def full(shape):
    return pl.BlockSpec(shape, lambda *_: (0,) * len(shape))


def spec(shape, at):
    return pl.BlockSpec(shape, at)


def body(
    tokens, norm_gain, rec_query, rec_input, rec_forward, rec_backward, forget_gap, log_decay,
    rec_gain, conv_value, conv_gate, conv_kernel, conv_gain, out_rec, out_conv,
):
    y, z = lax.axis_index(Y), lax.axis_index(Z)

    first = pl.pallas_call(
        first_kernel, out_shape=jax.ShapeDtypeStruct((8, 32, 896), BF16), name="first"
    )(
        rec_forward, rec_backward, rec_query, conv_value, conv_gate, rec_input, log_decay[0],
        out_rec.T, out_conv.T,
    )
    first = lax.all_to_all(first, Y, split_axis=0, concat_axis=0, tiled=True)
    normed = pl.pallas_call(
        norm_kernel, out_shape=jax.ShapeDtypeStruct((64, 2048), BF16), name="norm"
    )(tokens[0], norm_gain.reshape(1, 2048))
    seq = lax.all_gather(normed, (Y, C), axis=0, tiled=True)
    second, second2, out_cols, decays = pl.pallas_call(
        second_kernel,
        out_shape=[
            jax.ShapeDtypeStruct((224, 256), BF16),
            jax.ShapeDtypeStruct((8, 64, 256), BF16),
            jax.ShapeDtypeStruct((256, 512), BF16),
            jax.ShapeDtypeStruct((8, 2, 128), F32),
        ],
        name="second",
    )(first)
    weights2 = lax.all_to_all(second2, Z, split_axis=0, concat_axis=0, tiled=True)
    weights = lax.all_gather(second, Z, axis=0)
    out_w = lax.all_gather(out_cols, (C, Z), axis=0, tiled=True).reshape(2, 2048, 512)

    gains = lax.all_gather(jnp.stack([rec_gain, conv_gain]), C)
    rec_gains = gains[:, 0].reshape(4, 128)
    conv_gains = gains[:, 1].reshape(4, 128)
    gap = lax.dynamic_index_in_dim(forget_gap.reshape(2, 8, 32), y, 1, keepdims=False)
    gap = jnp.pad(gap.reshape(1, 64), ((0, 0), (0, 64)))
    taps = lax.dynamic_index_in_dim(conv_kernel.reshape(31, 8, 32), y, 1, keepdims=False)
    taps = jnp.pad(taps.astype(F32), ((0, 1), (0, 0)))

    n = seq.shape[0]
    tile = 256
    pre_a, pre_v, cum, gated, sent, before, offset = pl.pallas_call(
        states_kernel,
        grid=(n // tile,),
        in_specs=[
            spec((tile, 2048), lambda i: (i, 0)),
            full((8, 224, 256)),
            full((8, 64, 256)),
            spec((tile // 128, 2, 128), lambda i: (i, 0, 0)),
            full((1, 128)),
        ],
        out_specs=[
            spec((tile, 128), lambda i: (i, 0)),
            spec((tile, 128), lambda i: (i, 0)),
            spec((tile, 128), lambda i: (i, 0)),
            spec((tile, 32), lambda i: (i, 0)),
            full((8, 96, 128)),
            full((16, 64, 128)),
            full((16, 8, 128)),
        ],
        out_shape=[
            jax.ShapeDtypeStruct((n, 128), BF16),
            jax.ShapeDtypeStruct((n, 128), BF16),
            jax.ShapeDtypeStruct((n, 128), F32),
            jax.ShapeDtypeStruct((n, 32), BF16),
            jax.ShapeDtypeStruct((8, 96, 128), BF16),
            jax.ShapeDtypeStruct((16, 64, 128), BF16),
            jax.ShapeDtypeStruct((16, 8, 128), F32),
        ],
        scratch_shapes=[
            pltpu.VMEM((16, 64, 128), F32), pltpu.VMEM((16, 8, 128), F32), pltpu.VMEM((16, 128), F32)
        ],
        name="states",
    )(seq, weights, weights2, decays, gap)

    arrived = lax.all_to_all(sent, Z, split_axis=0, concat_axis=0, tiled=True)
    local, decayed, convolved, edges = pl.pallas_call(
        local_kernel,
        out_shape=[
            jax.ShapeDtypeStruct((n, 128), F32),
            jax.ShapeDtypeStruct((n, 128), BF16),
            jax.ShapeDtypeStruct((16, 16, 128), BF16),
            jax.ShapeDtypeStruct((2, 16, 32), F32),
        ],
        scratch_shapes=[pltpu.VMEM((n + 32, 32), F32)],
        name="local",
    )(pre_a, pre_v, cum, gap, before, offset, gated, taps)
    merged = pl.pallas_call(
        merge_kernel,
        in_specs=[pl.BlockSpec(memory_space=pltpu.SMEM)]
        + [pl.BlockSpec(memory_space=pltpu.VMEM)] * 6,
        out_shape=jax.ShapeDtypeStruct((16, 80, 128), BF16),
        name="merge",
    )(z.reshape(1).astype(jnp.int32), arrived, local, decayed, convolved, edges, taps)
    mine = lax.all_to_all(merged, (Y, C), split_axis=0, concat_axis=0, tiled=True)
    mixed = pl.pallas_call(
        output_kernel,
        grid=(4,),
        in_specs=[
            full((16, 80, 128)), full((4, 128)), full((4, 128)),
            spec((2, 512, 512), lambda i: (0, i, 0)),
        ],
        out_specs=spec((64, 512), lambda i: (0, i)),
        out_shape=jax.ShapeDtypeStruct((64, 2048), BF16),
        scratch_shapes=[pltpu.VMEM((64, 1024), BF16)],
        name="output",
    )(mine, rec_gains, conv_gains, out_w)
    return mixed[None]


def solution(mesh):
    finer = Mesh(
        mesh.devices.reshape(8, 8, mesh.shape["fs"], mesh.shape["tp"]), (Z, Y, X, C)
    )
    sp, sp_tp = (Z, Y), (Z, Y, C)
    row = P(sp, C)
    placed = (
        P(X, sp_tp, None), P(), row, row, row, row, P(None, C), P(X, None, C, sp), P(C),
        row, row, P(None, C), P(C), P(C, sp), P(C, sp),
    )
    return jax.shard_map(
        body, mesh=finer, in_specs=placed, out_specs=P(X, sp_tp, None), check_vma=False
    )
```

```python
import jax
import jax.numpy as jnp
from jax import lax
from jax.experimental import pallas as pl
from jax.experimental.pallas import tpu as pltpu
from jax.sharding import Mesh
from jax.sharding import PartitionSpec as P

KD = 128
BLOCK = 64
EPS = 1e-06
Z, Y, X, C = "sp_0", "sp_1", "fs", "tp"
F32, BF16 = jnp.float32, jnp.bfloat16
NN = (((1,), (0,)), ((), ()))
NT = (((1,), (1,)), ((), ()))
TN = (((0,), (0,)), ((), ()))


def dot(a, b, dims):
    return lax.dot_general(a, b, dims, preferred_element_type=F32)


def sigmoid(x):
    return 1.0 / (1.0 + jnp.exp(-x))


def lanes(rows):
    return lax.broadcasted_iota(jnp.int32, (rows, 128), 1)


def triangles():
    r = lax.broadcasted_iota(jnp.int32, (128, 128), 0)
    c = lax.broadcasted_iota(jnp.int32, (128, 128), 1)
    same = (r // BLOCK) == (c // BLOCK)
    return same & (c <= r), same & (c >= r)


def split_dot(mask, x):
    hi = x.astype(BF16)
    lo = (x - hi.astype(F32)).astype(BF16)
    return dot(mask, hi, NN) + dot(mask, lo, NN)


def gate_keys(a, gap):
    return gap * sigmoid(-a)


def start_kernel(
    x_ref, gain_ref, rf_ref, rb_ref, rq_ref, cv_ref, cg_ref, ri_ref, ld_ref, rec_ref, conv_ref,
    norm_ref, out_ref,
):
    for r in range(0, 64, 16):
        x = x_ref[r : r + 16, :].astype(F32)
        scale = lax.rsqrt(jnp.mean(x * x, axis=1, keepdims=True) + EPS)
        norm_ref[r : r + 16, :] = (x * scale * gain_ref[...]).astype(BF16)
    group = lanes(32) // 32
    row = lax.broadcasted_iota(jnp.int32, (32, 128), 0)
    for m in range(2):
        cols = slice(128 * m, 128 * (m + 1))
        src = [r[:, cols].astype(F32) for r in (rf_ref, rb_ref, rq_ref, cv_ref)]
        gate = cg_ref[:, cols].astype(F32)
        decays = jnp.zeros((32, 128), F32)
        for d in range(2):
            rest = jnp.broadcast_to(ld_ref[d, m : m + 1, :], (8, 128))
            for s in range(3):
                part = rest.astype(BF16).astype(F32)
                rest = rest - part
                low = pltpu.roll(part, 32, 1)[0:1]
                high = pltpu.roll(part, 64, 1)[0:1]
                decays = jnp.where(row == 2 * s + d, low, decays)
                decays = jnp.where(row == 6 + 2 * s + d, high, decays)
        for q in range(4):
            y = 4 * m + q
            a = jnp.zeros((32, 128), F32)
            for p in range(4):
                shift = (32 * (p - q)) % 128
                moved = pltpu.roll(src[p], shift, 1) if shift else src[p]
                a = jnp.where(group == p, moved, a)
            out_ref[y, :, 0:128] = a.astype(BF16)
            out_ref[y, :, 128:256] = ri_ref[:, cols]
            shift = (-32 * q) % 128
            moved = pltpu.roll(gate, shift, 1) if shift else gate
            out_ref[y, :, 256:384] = jnp.where(group == 0, moved, decays).astype(BF16)
            out_ref[y, :, 384:640] = rec_ref[...]
            out_ref[y, :, 640:896] = conv_ref[...]


def second_kernel(
    first_ref, gap_ref, taps_ref, w_ref, w2_ref, cols_ref, ld_ref, gap_out, taps_out
):
    gap_out[...] = gap_ref[...]
    taps_out[...] = taps_ref[...]
    lane = lanes(8)
    keys, values, gates = [], [], []
    for y in range(8):
        third = first_ref[y, :, 256:384].astype(F32)
        keys.append(first_ref[y, :, 0:128].astype(F32))
        values.append(first_ref[y, :, 128:256].astype(F32))
        gates.append(third)
        cols_ref[32 * y : 32 * (y + 1), :] = first_ref[y, :, 384:896]
        low = third[0:2] + third[2:4] + third[4:6]
        high = third[6:8] + third[8:10] + third[10:12]
        low = jnp.concatenate([low, low, low, low], axis=0)
        high = jnp.concatenate([high, high, high, high], axis=0)
        ld_ref[y] = jnp.where(lane < 96, pltpu.roll(low, 96, 1), pltpu.roll(high, 64, 1))[0:2]
    keys = jnp.concatenate(keys, axis=0).T.astype(BF16)
    w_ref[0:128, :] = jnp.concatenate(values, axis=0).T.astype(BF16)
    w_ref[128:224, :] = keys[0:96]
    gates = jnp.concatenate(gates, axis=0).T[0:32].astype(BF16)
    for i in range(8):
        w2_ref[i, 0:32, :] = keys[96:128]
        w2_ref[i, 32:64, :] = gates


def states_kernel(
    x_ref, w_ref, w2_ref, ld_ref, gap_ref,
    a_ref, v_ref, c_ref, gated_ref, send_ref, before_ref, offset_ref,
    chunk_s, chunk_t, edge,
):
    step = pl.program_id(0)
    rows = x_ref.shape[0]
    acc = jnp.zeros((rows, 224), F32)
    acc_g = jnp.zeros((rows, 64), F32)
    for k in range(8):
        xk = x_ref[:, 256 * k : 256 * (k + 1)]
        acc += dot(xk, w_ref[k], NT)
        acc_g += dot(xk, w2_ref[k], NT)
    pre_v = acc[:, :128].astype(BF16)
    pre_a = jnp.concatenate([acc[:, 128:], jnp.zeros((rows, 32), F32)], axis=1).astype(BF16)
    a_ref[...] = pre_a
    v_ref[...] = pre_v
    glu = acc_g.astype(BF16).astype(F32)
    gated = glu[:, 0:32] * sigmoid(glu[:, 32:64])
    gated_ref[...] = gated.astype(BF16)

    @pl.when(step == 0)
    def _():
        edge[...] = jnp.concatenate([gated[:16], gated[:16], gated[:16], gated[:16]], axis=1)

    @pl.when(step == pl.num_programs(0) - 1)
    def _():
        last = gated[rows - 16 :]
        last = jnp.concatenate([last, last, last, last], axis=1)
        edge[...] = jnp.where(lanes(16) < 32, edge[...], last)

    lower, upper = triangles()
    lower_f, upper_f = lower.astype(F32), upper.astype(F32)
    lower_b, upper_b = lower_f.astype(BF16), upper_f.astype(BF16)
    lane = lanes(128)
    lane1 = lanes(1)
    for b in range(rows // 128):
        a = pre_a[128 * b : 128 * (b + 1)].astype(F32)
        v = pre_v[128 * b : 128 * (b + 1)]
        k = gate_keys(a, gap_ref[...])
        g = jnp.log1p(-k)
        ld = ld_ref[b]
        cum_f = split_dot(lower_b, g) + jnp.sum(lower_f * ld[0:1], axis=1, keepdims=True)
        cum_b = split_dot(upper_b, g) + jnp.sum(upper_f * ld[1:2], axis=1, keepdims=True)
        cum = jnp.where(lane < 32, cum_f, cum_b)
        c_ref[128 * b : 128 * (b + 1), :] = cum
        for h in range(2):
            part = slice(64 * h, 64 * (h + 1))
            cc = cum[part]
            tot = jnp.where(lane1 < 32, cc[63:64], cc[0:1])
            kd = (k[part] * jnp.exp(tot - cc)).astype(BF16)
            st = dot(v[part], kd, TN)
            packed = st[:64] + pltpu.roll(st[64:], 64, 1)
            tot8 = jnp.broadcast_to(tot, (8, 128))
            tot8 = jnp.where(lanes(8) < 64, tot8, pltpu.roll(tot8, 64, 1))
            idx = step * (rows // 64) + 2 * b + h
            chunk_s[idx] = packed
            chunk_t[idx] = tot8

    @pl.when(step == pl.num_programs(0) - 1)
    def _():
        n = chunk_s.shape[0]
        fwd = (lanes(64) % 64) < 32
        fwd8 = (lanes(8) % 64) < 32
        s = jnp.zeros((64, 128), F32)
        off = jnp.zeros((8, 128), F32)
        befores, offs = [None] * n, [None] * n
        for i in range(n):
            j = n - 1 - i
            befores[i], offs[i] = s, off
            tt = jnp.where(fwd8, chunk_t[i], chunk_t[j])
            sc = jnp.where(fwd, chunk_s[i], chunk_s[j])
            s = s * jnp.exp(tt)[0:1] + sc
            off = off + tt
        for i in range(n):
            j = n - 1 - i
            before_ref[i] = jnp.where(fwd, befores[i], befores[j]).astype(BF16)
            offset_ref[i] = jnp.where(fwd8, offs[i], offs[j])
        dec = jnp.exp(off)[0:1]
        hi = dec.astype(BF16)
        lo = (dec - hi.astype(F32)).astype(BF16)
        row = lax.broadcasted_iota(jnp.int32, (16, 128), 0)
        tail = jnp.where(row == 0, hi.astype(F32), jnp.where(row == 1, lo.astype(F32), 0.0))
        s = s.astype(BF16)
        tail = tail.astype(BF16)
        for i in range(8):
            send_ref[i, :64, :] = s
            send_ref[i, 64:80, :] = tail
            send_ref[i, 80:96, :] = edge[...].astype(BF16)


def local_kernel(
    a_ref, v_ref, c_ref, gap_ref, before_ref, offset_ref, g_ref, taps_ref,
    out_ref, qd_ref, conv_ref, edge_ref, pad,
):
    n = g_ref.shape[0]
    zeros = jnp.zeros((16, 32), F32)
    pad[0:16, :] = zeros
    pad[16 : 16 + n, :] = g_ref[...].astype(F32)
    pad[16 + n : 32 + n, :] = zeros
    taps = taps_ref[...]
    for blk in range(n // 64):
        acc = jnp.zeros((64, 32), F32)
        for j in range(31):
            acc += pad[64 * blk + j + 1 : 64 * blk + j + 65, :] * taps[j : j + 1, :]
        conv_ref[blk] = jnp.concatenate([acc[16 * q : 16 * (q + 1)] for q in range(4)], axis=1).astype(BF16)
        if blk == 0:
            edge_ref[0] = acc[0:16]
        if blk == n // 64 - 1:
            edge_ref[1] = acc[48:64]
    lower, upper = triangles()
    lane = lanes(128)
    for b in range(a_ref.shape[0] // 128):
        rows = slice(128 * b, 128 * (b + 1))
        a = a_ref[rows, :].astype(F32)
        v = v_ref[rows, :]
        cum = c_ref[rows, :]
        k = gate_keys(a, gap_ref[...])
        q = a * sigmoid(a) * (KD ** -0.5)
        q = jnp.where(lane < 32, pltpu.roll(q, 64, 1), pltpu.roll(q, 96, 1))
        q = jnp.where(lane < 64, q, 0.0)
        qg = q * jnp.exp(cum)
        kn = (k * jnp.exp(-cum)).astype(BF16)
        qf = jnp.where(lane < 32, qg, 0.0).astype(BF16)
        qb = jnp.where(lane < 32, 0.0, qg).astype(BF16)
        qh = qg.astype(BF16)
        scores = jnp.where(lower, dot(qf, kn, NT), 0.0) + jnp.where(upper, dot(qb, kn, NT), 0.0)
        out = dot(scores.astype(BF16), v, NN)
        for h in range(2):
            part = slice(64 * h, 64 * (h + 1))
            to = slice(128 * b + 64 * h, 128 * b + 64 * (h + 1))
            sb = before_ref[2 * b + h]
            full = jnp.concatenate([sb, pltpu.roll(sb.astype(F32), 64, 1).astype(BF16)], axis=0)
            out_ref[to, :] = out[part] + dot(qh[part], full, NT)
            qd_ref[to, :] = (qg[part] * jnp.exp(offset_ref[2 * b + h][0:1])).astype(BF16)


def merge_kernel(z_ref, recv_ref, local_ref, qd_ref, conv_ref, edge_ref, taps_ref, send_ref):
    z = z_ref[0]
    heads = jnp.zeros((16, 128), F32)
    tails = jnp.zeros((16, 128), F32)
    for i in range(8):
        other = recv_ref[i, 80:96, :].astype(F32)
        tails = jnp.where(i == z - 1, other, tails)
        heads = jnp.where(i == z + 1, other, heads)
    zeros = jnp.zeros((16, 32), F32)
    before = jnp.concatenate([tails[:, 32:64], zeros], axis=0)
    after = jnp.concatenate([zeros, heads[:, 0:32]], axis=0)
    first, last = edge_ref[0], edge_ref[1]
    taps = taps_ref[...]
    for j in range(15):
        first += before[j + 1 : j + 17] * taps[j : j + 1, :]
        last += after[j + 1 : j + 17] * taps[16 + j : 17 + j, :]
    first = jnp.concatenate([first] * 4, axis=1).astype(BF16)
    last = jnp.concatenate([last] * 4, axis=1).astype(BF16)
    lane16 = lanes(16)
    fwd = (lanes(64) % 64) < 32
    fwd1 = (lanes(1) % 64) < 32
    s = jnp.zeros((64, 128), F32)
    for i in range(8):
        j = 7 - i
        sc = jnp.where(fwd, recv_ref[i, :64, :].astype(F32), recv_ref[j, :64, :].astype(F32))
        di = recv_ref[i, 64:80, :].astype(F32)
        dj = recv_ref[j, 64:80, :].astype(F32)
        dec = jnp.where(fwd1, di[0:1] + di[1:2], dj[0:1] + dj[1:2])
        pass_f = jnp.where(i < z, 1, 0)
        pass_b = jnp.where(j > z, 1, 0)
        passed = jnp.where(fwd, pass_f, pass_b) > 0
        s = jnp.where(passed, s * dec + sc, s)
    full = jnp.concatenate([s, pltpu.roll(s, 64, 1)], axis=0).astype(BF16)
    for blk in range(16):
        rows = slice(64 * blk, 64 * (blk + 1))
        out = local_ref[rows, :] + dot(qd_ref[rows, :], full, NT)
        send_ref[blk, :64, :] = out.astype(BF16)
        packed = conv_ref[blk]
        if blk == 0:
            packed = jnp.where(lane16 < 32, first, packed)
        if blk == 15:
            packed = jnp.where(lane16 >= 96, last, packed)
        send_ref[blk, 64:, :] = packed


def output_kernel(recv_ref, rec_gain_ref, conv_gain_ref, w_ref, out_ref, act):
    @pl.when(pl.program_id(0) == 0)
    def _():
        for c in range(2):
            for h in range(2):
                rec = sum(recv_ref[(4 * h + q) * 2 + c, :64, :].astype(F32) for q in range(4))
                rec = rec * lax.rsqrt(jnp.mean(rec * rec, axis=1, keepdims=True) + EPS)
                rec = rec * rec_gain_ref[2 * c + h : 2 * c + h + 1, :]
                at = 128 * (4 * c + h)
                act[:, at : at + 128] = rec.astype(BF16)
        lane = lanes(16) // 32
        blocks = []
        for c in range(2):
            for m in range(2):
                parts = [recv_ref[(4 * m + q) * 2 + c, 64:80, :].astype(F32) for q in range(4)]
                groups = []
                for g in range(4):
                    value = jnp.zeros((16, 128), F32)
                    for q in range(4):
                        moved = parts[q] if q == g else pltpu.roll(parts[q], (32 * (q - g)) % 128, 1)
                        value = jnp.where(lane == q, moved, value)
                    groups.append(value)
                blocks.append(jnp.concatenate(groups, axis=0))
        total = sum(jnp.sum(b, axis=1, keepdims=True) for b in blocks)
        square = sum(jnp.sum(b * b, axis=1, keepdims=True) for b in blocks)
        mean = total / 512.0
        scale = lax.rsqrt(square / 512.0 - mean * mean + EPS)
        for c in range(2):
            for m in range(2):
                n = 2 * c + m
                y = (blocks[n] - mean) * scale * conv_gain_ref[n : n + 1, :]
                at = 128 * (4 * c + 2 + m)
                act[:, at : at + 128] = (y * sigmoid(y)).astype(BF16)

    acc = jnp.zeros(out_ref.shape, F32)
    for c in range(2):
        acc += dot(act[:, 512 * c : 512 * (c + 1)], w_ref[c], NT)
    out_ref[...] = acc.astype(BF16)


def near(x):
    return pltpu.with_memory_space_constraint(x, pltpu.VMEM)


def kept(shape, dtype):
    return pltpu.VMEM(shape, dtype)


def full(shape):
    return pl.BlockSpec(shape, lambda *_: (0,) * len(shape))


def spec(shape, at):
    return pl.BlockSpec(shape, at)


def body(
    tokens, norm_gain, rec_query, rec_input, rec_forward, rec_backward, forget_gap, log_decay,
    rec_gain, conv_value, conv_gate, conv_kernel, conv_gain, out_rec, out_conv,
):
    y, z = lax.axis_index(Y), lax.axis_index(Z)

    gap = lax.dynamic_index_in_dim(forget_gap.reshape(2, 8, 32), y, 1, keepdims=False)
    gap = jnp.pad(gap.reshape(1, 64), ((0, 0), (0, 64)))
    taps = lax.dynamic_index_in_dim(conv_kernel.reshape(31, 8, 32), y, 1, keepdims=False)
    taps = jnp.pad(taps.astype(F32), ((0, 1), (0, 0)))
    normed, first = pl.pallas_call(
        start_kernel,
        out_shape=[kept((64, 2048), BF16), kept((8, 32, 896), BF16)],
        name="start",
    )(
        tokens[0], norm_gain.reshape(1, 2048), rec_forward, rec_backward, rec_query, conv_value,
        conv_gate, rec_input, log_decay[0], out_rec.T, out_conv.T,
    )
    seq = lax.all_gather(normed, (Y, C), axis=0, tiled=True)
    first = lax.all_to_all(first, Y, split_axis=0, concat_axis=0, tiled=True)
    second, second2, out_cols, decays, gap, taps = pl.pallas_call(
        second_kernel,
        out_shape=[
            kept((224, 256), BF16),
            kept((8, 64, 256), BF16),
            jax.ShapeDtypeStruct((256, 512), BF16),
            kept((8, 2, 128), F32),
            kept((1, 128), F32),
            kept((32, 32), F32),
        ],
        name="second",
    )(near(first), near(gap), near(taps))
    weights2 = lax.all_to_all(second2, Z, split_axis=0, concat_axis=0, tiled=True)
    weights = lax.all_gather(second, Z, axis=0)
    out_w = lax.all_gather(out_cols, (C, Z), axis=0, tiled=True).reshape(2, 2048, 512)

    gains = lax.all_gather(jnp.stack([rec_gain, conv_gain]), C)
    rec_gains = gains[:, 0].reshape(4, 128)
    conv_gains = gains[:, 1].reshape(4, 128)
    n = seq.shape[0]
    tile = 256
    pre_a, pre_v, cum, gated, sent, before, offset = pl.pallas_call(
        states_kernel,
        grid=(n // tile,),
        in_specs=[
            spec((tile, 2048), lambda i: (i, 0)),
            full((8, 224, 256)),
            full((8, 64, 256)),
            spec((tile // 128, 2, 128), lambda i: (i, 0, 0)),
            full((1, 128)),
        ],
        out_specs=[
            spec((tile, 128), lambda i: (i, 0)),
            spec((tile, 128), lambda i: (i, 0)),
            spec((tile, 128), lambda i: (i, 0)),
            spec((tile, 32), lambda i: (i, 0)),
            full((8, 96, 128)),
            full((16, 64, 128)),
            full((16, 8, 128)),
        ],
        out_shape=[
            jax.ShapeDtypeStruct((n, 128), BF16),
            jax.ShapeDtypeStruct((n, 128), BF16),
            jax.ShapeDtypeStruct((n, 128), F32),
            jax.ShapeDtypeStruct((n, 32), BF16),
            jax.ShapeDtypeStruct((8, 96, 128), BF16),
            jax.ShapeDtypeStruct((16, 64, 128), BF16),
            jax.ShapeDtypeStruct((16, 8, 128), F32),
        ],
        scratch_shapes=[
            pltpu.VMEM((16, 64, 128), F32), pltpu.VMEM((16, 8, 128), F32), pltpu.VMEM((16, 128), F32)
        ],
        name="states",
    )(seq, near(weights), near(weights2), near(decays), near(gap))

    arrived = lax.all_to_all(sent, Z, split_axis=0, concat_axis=0, tiled=True)
    local, decayed, convolved, edges = pl.pallas_call(
        local_kernel,
        out_shape=[
            kept((n, 128), F32),
            kept((n, 128), BF16),
            kept((16, 16, 128), BF16),
            kept((2, 16, 32), F32),
        ],
        scratch_shapes=[pltpu.VMEM((n + 32, 32), F32)],
        name="local",
    )(near(pre_a), near(pre_v), near(cum), near(gap), near(before), near(offset), near(gated), near(taps))
    merged = pl.pallas_call(
        merge_kernel,
        in_specs=[pl.BlockSpec(memory_space=pltpu.SMEM)]
        + [pl.BlockSpec(memory_space=pltpu.VMEM)] * 6,
        out_shape=kept((16, 80, 128), BF16),
        name="merge",
    )(z.reshape(1).astype(jnp.int32), near(arrived), near(local), near(decayed), near(convolved), near(edges), near(taps))
    mine = lax.all_to_all(merged, (Y, C), split_axis=0, concat_axis=0, tiled=True)
    mixed = pl.pallas_call(
        output_kernel,
        grid=(4,),
        in_specs=[
            full((16, 80, 128)), full((4, 128)), full((4, 128)),
            spec((2, 512, 512), lambda i: (0, i, 0)),
        ],
        out_specs=spec((64, 512), lambda i: (0, i)),
        out_shape=jax.ShapeDtypeStruct((64, 2048), BF16),
        scratch_shapes=[pltpu.VMEM((64, 1024), BF16)],
        name="output",
    )(near(mine), rec_gains, conv_gains, out_w)
    return mixed[None]


def solution(mesh):
    finer = Mesh(
        mesh.devices.reshape(8, 8, mesh.shape["fs"], mesh.shape["tp"]), (Z, Y, X, C)
    )
    sp, sp_tp = (Z, Y), (Z, Y, C)
    row = P(sp, C)
    placed = (
        P(X, sp_tp, None), P(), row, row, row, row, P(None, C), P(X, None, C, sp), P(C),
        row, row, P(None, C), P(C), P(C, sp), P(C, sp),
    )
    return jax.shard_map(
        body, mesh=finer, in_specs=placed, out_specs=P(X, sp_tp, None), check_vma=False
    )
```

```python
import jax
import jax.numpy as jnp
from jax import lax
from jax.experimental import pallas as pl
from jax.experimental.pallas import tpu as pltpu
from jax.sharding import Mesh
from jax.sharding import PartitionSpec as P

KD = 128
BLOCK = 64
TILE = 256
SMALL = pltpu.CompilerParams(vmem_limit_bytes=24 * 1024 * 1024)
EPS = 1e-06
Z, Y, X, C = "sp_0", "sp_1", "fs", "tp"
F32, BF16 = jnp.float32, jnp.bfloat16
NN = (((1,), (0,)), ((), ()))
NT = (((1,), (1,)), ((), ()))
TN = (((0,), (0,)), ((), ()))


def dot(a, b, dims):
    return lax.dot_general(a, b, dims, preferred_element_type=F32)


def sigmoid(x):
    return 1.0 / (1.0 + jnp.exp(-x))


def lanes(rows):
    return lax.broadcasted_iota(jnp.int32, (rows, 128), 1)


def triangles():
    r = lax.broadcasted_iota(jnp.int32, (128, 128), 0)
    c = lax.broadcasted_iota(jnp.int32, (128, 128), 1)
    same = (r // BLOCK) == (c // BLOCK)
    return same & (c <= r), same & (c >= r)


def split_dot(mask, x):
    hi = x.astype(BF16)
    lo = (x - hi.astype(F32)).astype(BF16)
    return dot(mask, hi, NN) + dot(mask, lo, NN)


def gate_keys(a, gap):
    return gap * sigmoid(-a)


def start_kernel(
    x_ref, gain_ref, rf_ref, rb_ref, rq_ref, cv_ref, cg_ref, ri_ref, ld_ref, rec_ref, conv_ref,
    norm_ref, out_ref,
):
    for r in range(0, 64, 16):
        x = x_ref[r : r + 16, :].astype(F32)
        scale = lax.rsqrt(jnp.mean(x * x, axis=1, keepdims=True) + EPS)
        norm_ref[r : r + 16, :] = (x * scale * gain_ref[...]).astype(BF16)
    group = lanes(32) // 32
    row = lax.broadcasted_iota(jnp.int32, (32, 128), 0)
    for m in range(2):
        cols = slice(128 * m, 128 * (m + 1))
        src = [r[:, cols].astype(F32) for r in (rf_ref, rb_ref, rq_ref, cv_ref)]
        gate = cg_ref[:, cols].astype(F32)
        decays = jnp.zeros((32, 128), F32)
        for d in range(2):
            rest = jnp.broadcast_to(ld_ref[d, m : m + 1, :], (8, 128))
            for s in range(3):
                part = rest.astype(BF16).astype(F32)
                rest = rest - part
                low = pltpu.roll(part, 32, 1)[0:1]
                high = pltpu.roll(part, 64, 1)[0:1]
                decays = jnp.where(row == 2 * s + d, low, decays)
                decays = jnp.where(row == 6 + 2 * s + d, high, decays)
        for q in range(4):
            y = 4 * m + q
            a = jnp.zeros((32, 128), F32)
            for p in range(4):
                shift = (32 * (p - q)) % 128
                moved = pltpu.roll(src[p], shift, 1) if shift else src[p]
                a = jnp.where(group == p, moved, a)
            out_ref[y, :, 0:128] = a.astype(BF16)
            out_ref[y, :, 128:256] = ri_ref[:, cols]
            shift = (-32 * q) % 128
            moved = pltpu.roll(gate, shift, 1) if shift else gate
            out_ref[y, :, 256:384] = jnp.where(group == 0, moved, decays).astype(BF16)
            out_ref[y, :, 384:640] = rec_ref[...]
            out_ref[y, :, 640:896] = conv_ref[...]


def second_kernel(
    first_ref, gap_ref, taps_ref, w_ref, w2_ref, cols_ref, ld_ref, gap_out, taps_out
):
    gap_out[...] = gap_ref[...]
    taps_out[...] = taps_ref[...]
    lane = lanes(8)
    keys, values, gates = [], [], []
    for y in range(8):
        third = first_ref[y, :, 256:384].astype(F32)
        keys.append(first_ref[y, :, 0:128].astype(F32))
        values.append(first_ref[y, :, 128:256].astype(F32))
        gates.append(third)
        cols_ref[32 * y : 32 * (y + 1), :] = first_ref[y, :, 384:896]
        low = third[0:2] + third[2:4] + third[4:6]
        high = third[6:8] + third[8:10] + third[10:12]
        low = jnp.concatenate([low, low, low, low], axis=0)
        high = jnp.concatenate([high, high, high, high], axis=0)
        ld_ref[y] = jnp.where(lane < 96, pltpu.roll(low, 96, 1), pltpu.roll(high, 64, 1))[0:2]
    keys = jnp.concatenate(keys, axis=0).T.astype(BF16)
    w_ref[0:128, :] = jnp.concatenate(values, axis=0).T.astype(BF16)
    w_ref[128:224, :] = keys[0:96]
    gates = jnp.concatenate(gates, axis=0).T[0:32].astype(BF16)
    for i in range(8):
        w2_ref[i, 0:32, :] = keys[96:128]
        w2_ref[i, 32:64, :] = gates


def states_kernel(
    x_hbm, w_ref, w2_ref, ld_ref, gap_ref,
    a_ref, v_ref, c_ref, gated_ref, send_ref, before_ref, offset_ref,
    x_ref, sems, chunk_s, chunk_t,
):
    rows = TILE
    n = x_ref.shape[0] // 64
    copies = []
    for t in range(x_ref.shape[0] // rows):
        at = pl.ds(rows * t, rows)
        copies.append(pltpu.make_async_copy(x_hbm.at[at], x_ref.at[at], sems.at[t]))
        copies[-1].start()
    lower, upper = triangles()
    lower_f, upper_f = lower.astype(F32), upper.astype(F32)
    lower_b, upper_b = lower_f.astype(BF16), upper_f.astype(BF16)
    lane = lanes(128)
    lane1 = lanes(1)
    for t, copy in enumerate(copies):
        copy.wait()
        start = rows * t
        acc = jnp.zeros((rows, 224), F32)
        acc_g = jnp.zeros((rows, 64), F32)
        for k in range(8):
            xk = x_ref[start : start + rows, 256 * k : 256 * (k + 1)]
            acc += dot(xk, w_ref[k], NT)
            acc_g += dot(xk, w2_ref[k], NT)
        pre_v = acc[:, :128].astype(BF16)
        pre_a = jnp.concatenate([acc[:, 128:], jnp.zeros((rows, 32), F32)], axis=1).astype(BF16)
        a_ref[start : start + rows, :] = pre_a
        v_ref[start : start + rows, :] = pre_v
        glu = acc_g.astype(BF16).astype(F32)
        gated_ref[start : start + rows, :] = (glu[:, 0:32] * sigmoid(glu[:, 32:64])).astype(BF16)
        for b in range(rows // 128):
            a = pre_a[128 * b : 128 * (b + 1)].astype(F32)
            v = pre_v[128 * b : 128 * (b + 1)]
            k = gate_keys(a, gap_ref[...])
            g = jnp.log1p(-k)
            ld = ld_ref[t * (rows // 128) + b]
            cum_f = split_dot(lower_b, g) + jnp.sum(lower_f * ld[0:1], axis=1, keepdims=True)
            cum_b = split_dot(upper_b, g) + jnp.sum(upper_f * ld[1:2], axis=1, keepdims=True)
            cum = jnp.where(lane < 32, cum_f, cum_b)
            c_ref[start + 128 * b : start + 128 * (b + 1), :] = cum
            for h in range(2):
                part = slice(64 * h, 64 * (h + 1))
                cc = cum[part]
                tot = jnp.where(lane1 < 32, cc[63:64], cc[0:1])
                kd = (k[part] * jnp.exp(tot - cc)).astype(BF16)
                st = dot(v[part], kd, TN)
                tot8 = jnp.broadcast_to(tot, (8, 128))
                tot8 = jnp.where(lanes(8) < 64, tot8, pltpu.roll(tot8, 64, 1))
                idx = t * (rows // 64) + 2 * b + h
                chunk_s[idx] = st[:64] + pltpu.roll(st[64:], 64, 1)
                chunk_t[idx] = tot8

    fwd = (lanes(64) % 64) < 32
    fwd8 = (lanes(8) % 64) < 32
    s = jnp.zeros((64, 128), F32)
    off = jnp.zeros((8, 128), F32)
    befores, offs = [None] * n, [None] * n
    for i in range(n):
        j = n - 1 - i
        befores[i], offs[i] = s, off
        tt = jnp.where(fwd8, chunk_t[i], chunk_t[j])
        sc = jnp.where(fwd, chunk_s[i], chunk_s[j])
        s = s * jnp.exp(tt)[0:1] + sc
        off = off + tt
        if i >= n // 2:
            for p, q in ((i, j), (j, i)):
                before_ref[p] = jnp.where(fwd, befores[p], befores[q]).astype(BF16)
                offset_ref[p] = jnp.where(fwd8, offs[p], offs[q])
    dec = jnp.exp(off)[0:1]
    hi = dec.astype(BF16)
    lo = (dec - hi.astype(F32)).astype(BF16)
    row = lax.broadcasted_iota(jnp.int32, (16, 128), 0)
    tail = jnp.where(row == 0, hi.astype(F32), jnp.where(row == 1, lo.astype(F32), 0.0)).astype(BF16)
    s = s.astype(BF16)
    head = gated_ref[0:16, :].astype(F32)
    last = gated_ref[gated_ref.shape[0] - 16 :, :].astype(F32)
    edge = jnp.concatenate([head, last, last, last], axis=1).astype(BF16)
    for i in range(8):
        send_ref[i, :64, :] = s
        send_ref[i, 64:80, :] = tail
        send_ref[i, 80:96, :] = edge


def local_kernel(
    a_ref, v_ref, c_ref, gap_ref, before_ref, offset_ref, g_ref, taps_ref,
    out_ref, qd_ref, conv_ref, edge_ref, pad,
):
    n = g_ref.shape[0]
    zeros = jnp.zeros((16, 32), F32)
    pad[0:16, :] = zeros
    pad[16 : 16 + n, :] = g_ref[...].astype(F32)
    pad[16 + n : 32 + n, :] = zeros
    taps = taps_ref[...]
    for blk in range(n // 64):
        acc = jnp.zeros((64, 32), F32)
        for j in range(31):
            acc += pad[64 * blk + j + 1 : 64 * blk + j + 65, :] * taps[j : j + 1, :]
        conv_ref[blk] = jnp.concatenate([acc[16 * q : 16 * (q + 1)] for q in range(4)], axis=1).astype(BF16)
        if blk == 0:
            edge_ref[0] = acc[0:16]
        if blk == n // 64 - 1:
            edge_ref[1] = acc[48:64]
    lower, upper = triangles()
    lane = lanes(128)
    for b in range(a_ref.shape[0] // 128):
        rows = slice(128 * b, 128 * (b + 1))
        a = a_ref[rows, :].astype(F32)
        v = v_ref[rows, :]
        cum = c_ref[rows, :]
        k = gate_keys(a, gap_ref[...])
        q = a * sigmoid(a) * (KD ** -0.5)
        q = jnp.where(lane < 32, pltpu.roll(q, 64, 1), pltpu.roll(q, 96, 1))
        q = jnp.where(lane < 64, q, 0.0)
        qg = q * jnp.exp(cum)
        kn = (k * jnp.exp(-cum)).astype(BF16)
        qf = jnp.where(lane < 32, qg, 0.0).astype(BF16)
        qb = jnp.where(lane < 32, 0.0, qg).astype(BF16)
        qh = qg.astype(BF16)
        scores = jnp.where(lower, dot(qf, kn, NT), 0.0) + jnp.where(upper, dot(qb, kn, NT), 0.0)
        out = dot(scores.astype(BF16), v, NN)
        for h in range(2):
            part = slice(64 * h, 64 * (h + 1))
            to = slice(128 * b + 64 * h, 128 * b + 64 * (h + 1))
            sb = before_ref[2 * b + h]
            full = jnp.concatenate([sb, pltpu.roll(sb.astype(F32), 64, 1).astype(BF16)], axis=0)
            out_ref[to, :] = out[part] + dot(qh[part], full, NT)
            qd_ref[to, :] = (qg[part] * jnp.exp(offset_ref[2 * b + h][0:1])).astype(BF16)


def merge_kernel(z_ref, recv_ref, local_ref, qd_ref, conv_ref, edge_ref, taps_ref, send_ref):
    z = z_ref[0]
    heads = jnp.zeros((16, 128), F32)
    tails = jnp.zeros((16, 128), F32)
    for i in range(8):
        other = recv_ref[i, 80:96, :].astype(F32)
        tails = jnp.where(i == z - 1, other, tails)
        heads = jnp.where(i == z + 1, other, heads)
    zeros = jnp.zeros((16, 32), F32)
    before = jnp.concatenate([tails[:, 32:64], zeros], axis=0)
    after = jnp.concatenate([zeros, heads[:, 0:32]], axis=0)
    first, last = edge_ref[0], edge_ref[1]
    taps = taps_ref[...]
    for j in range(15):
        first += before[j + 1 : j + 17] * taps[j : j + 1, :]
        last += after[j + 1 : j + 17] * taps[16 + j : 17 + j, :]
    first = jnp.concatenate([first] * 4, axis=1).astype(BF16)
    last = jnp.concatenate([last] * 4, axis=1).astype(BF16)
    lane16 = lanes(16)
    fwd = (lanes(64) % 64) < 32
    fwd1 = (lanes(1) % 64) < 32
    s = jnp.zeros((64, 128), F32)
    for i in range(8):
        j = 7 - i
        sc = jnp.where(fwd, recv_ref[i, :64, :].astype(F32), recv_ref[j, :64, :].astype(F32))
        di = recv_ref[i, 64:80, :].astype(F32)
        dj = recv_ref[j, 64:80, :].astype(F32)
        dec = jnp.where(fwd1, di[0:1] + di[1:2], dj[0:1] + dj[1:2])
        pass_f = jnp.where(i < z, 1, 0)
        pass_b = jnp.where(j > z, 1, 0)
        passed = jnp.where(fwd, pass_f, pass_b) > 0
        s = jnp.where(passed, s * dec + sc, s)
    full = jnp.concatenate([s, pltpu.roll(s, 64, 1)], axis=0).astype(BF16)
    for blk in range(16):
        rows = slice(64 * blk, 64 * (blk + 1))
        out = local_ref[rows, :] + dot(qd_ref[rows, :], full, NT)
        send_ref[blk, :64, :] = out.astype(BF16)
        packed = conv_ref[blk]
        if blk == 0:
            packed = jnp.where(lane16 < 32, first, packed)
        if blk == 15:
            packed = jnp.where(lane16 >= 96, last, packed)
        send_ref[blk, 64:, :] = packed


def output_kernel(
    recv_ref, rec_gain_ref, conv_gain_ref, w0_ref, w_hbm, out_ref, act, w1_ref, sem
):
    copy = pltpu.make_async_copy(w_hbm.at[1], w1_ref, sem)
    copy.start()
    for c in range(2):
        for h in range(2):
            rec = sum(recv_ref[(4 * h + q) * 2 + c, :64, :].astype(F32) for q in range(4))
            rec = rec * lax.rsqrt(jnp.mean(rec * rec, axis=1, keepdims=True) + EPS)
            rec = rec * rec_gain_ref[2 * c + h : 2 * c + h + 1, :]
            at = 128 * (4 * c + h)
            act[:, at : at + 128] = rec.astype(BF16)
    lane = lanes(16) // 32
    blocks = []
    for c in range(2):
        for m in range(2):
            parts = [recv_ref[(4 * m + q) * 2 + c, 64:80, :].astype(F32) for q in range(4)]
            groups = []
            for g in range(4):
                value = jnp.zeros((16, 128), F32)
                for q in range(4):
                    moved = parts[q] if q == g else pltpu.roll(parts[q], (32 * (q - g)) % 128, 1)
                    value = jnp.where(lane == q, moved, value)
                groups.append(value)
            blocks.append(jnp.concatenate(groups, axis=0))
    total = sum(jnp.sum(b, axis=1, keepdims=True) for b in blocks)
    square = sum(jnp.sum(b * b, axis=1, keepdims=True) for b in blocks)
    mean = total / 512.0
    scale = lax.rsqrt(square / 512.0 - mean * mean + EPS)
    for c in range(2):
        for m in range(2):
            n = 2 * c + m
            y = (blocks[n] - mean) * scale * conv_gain_ref[n : n + 1, :]
            at = 128 * (4 * c + 2 + m)
            act[:, at : at + 128] = (y * sigmoid(y)).astype(BF16)

    half = dot(act[:, 0:512], w0_ref[...], NT)
    copy.wait()
    out_ref[...] = (half + dot(act[:, 512:1024], w1_ref[...], NT)).astype(BF16)


def load_kernel(w_hbm, w_ref, sem):
    copy = pltpu.make_async_copy(w_hbm.at[0], w_ref, sem)
    copy.start()
    copy.wait()


def near(x):
    return pltpu.with_memory_space_constraint(x, pltpu.VMEM)


def kept(shape, dtype):
    return pltpu.VMEM(shape, dtype)


def body(
    tokens, norm_gain, rec_query, rec_input, rec_forward, rec_backward, forget_gap, log_decay,
    rec_gain, conv_value, conv_gate, conv_kernel, conv_gain, out_rec, out_conv,
):
    y, z = lax.axis_index(Y), lax.axis_index(Z)

    gap = lax.dynamic_index_in_dim(forget_gap.reshape(2, 8, 32), y, 1, keepdims=False)
    gap = jnp.pad(gap.reshape(1, 64), ((0, 0), (0, 64)))
    taps = lax.dynamic_index_in_dim(conv_kernel.reshape(31, 8, 32), y, 1, keepdims=False)
    taps = jnp.pad(taps.astype(F32), ((0, 1), (0, 0)))
    normed, first = pl.pallas_call(
        start_kernel,
        out_shape=[kept((64, 2048), BF16), kept((8, 32, 896), BF16)],
        name="start",
    )(
        tokens[0], norm_gain.reshape(1, 2048), rec_forward, rec_backward, rec_query, conv_value,
        conv_gate, rec_input, log_decay[0], out_rec.T, out_conv.T,
    )
    seq = lax.all_gather(normed, (Y, C), axis=0, tiled=True)
    first = lax.all_to_all(first, Y, split_axis=0, concat_axis=0, tiled=True)
    second, second2, out_cols, decays, gap, taps = pl.pallas_call(
        second_kernel,
        out_shape=[
            kept((224, 256), BF16),
            kept((8, 64, 256), BF16),
            jax.ShapeDtypeStruct((256, 512), BF16),
            kept((8, 2, 128), F32),
            kept((1, 128), F32),
            kept((32, 32), F32),
        ],
        name="second",
    )(near(first), near(gap), near(taps))
    weights2 = lax.all_to_all(second2, Z, split_axis=0, concat_axis=0, tiled=True)
    weights = lax.all_gather(second, Z, axis=0)
    out_w = lax.all_gather(out_cols, (C, Z), axis=0, tiled=True).reshape(2, 2048, 512)

    gains = lax.all_gather(jnp.stack([rec_gain, conv_gain]), C)
    rec_gains = gains[:, 0].reshape(4, 128)
    conv_gains = gains[:, 1].reshape(4, 128)
    n = seq.shape[0]
    pre_a, pre_v, cum, gated, sent, before, offset = pl.pallas_call(
        states_kernel,
        in_specs=[pl.BlockSpec(memory_space=pltpu.HBM)]
        + [pl.BlockSpec(memory_space=pltpu.VMEM)] * 4,
        out_shape=[
            kept((n, 128), BF16),
            kept((n, 128), BF16),
            kept((n, 128), F32),
            kept((n, 32), BF16),
            kept((8, 96, 128), BF16),
            kept((16, 64, 128), BF16),
            kept((16, 8, 128), F32),
        ],
        scratch_shapes=[
            pltpu.VMEM((n, 2048), BF16), pltpu.SemaphoreType.DMA((n // TILE,)),
            pltpu.VMEM((16, 64, 128), F32), pltpu.VMEM((16, 8, 128), F32),
        ],
        compiler_params=SMALL, name="states",
    )(pltpu.with_memory_space_constraint(seq, pltpu.HBM), near(weights), near(weights2), near(decays), near(gap))

    arrived = lax.all_to_all(sent, Z, split_axis=0, concat_axis=0, tiled=True)
    local, decayed, convolved, edges = pl.pallas_call(
        local_kernel,
        out_shape=[
            kept((n, 128), F32),
            kept((n, 128), BF16),
            kept((16, 16, 128), BF16),
            kept((2, 16, 32), F32),
        ],
        scratch_shapes=[pltpu.VMEM((n + 32, 32), F32)],
        compiler_params=SMALL, name="local",
    )(near(pre_a), near(pre_v), near(cum), near(gap), near(before), near(offset), near(gated), near(taps))
    merged = pl.pallas_call(
        merge_kernel,
        in_specs=[pl.BlockSpec(memory_space=pltpu.SMEM)]
        + [pl.BlockSpec(memory_space=pltpu.VMEM)] * 6,
        out_shape=kept((16, 80, 128), BF16),
        compiler_params=SMALL, name="merge",
    )(z.reshape(1).astype(jnp.int32), near(arrived), near(local), near(decayed), near(convolved), near(edges), near(taps))
    mine = lax.all_to_all(merged, (Y, C), split_axis=0, concat_axis=0, tiled=True)
    out_w = pltpu.with_memory_space_constraint(out_w, pltpu.HBM)
    out_w0 = pl.pallas_call(
        load_kernel,
        in_specs=[pl.BlockSpec(memory_space=pltpu.HBM)],
        out_shape=kept((2048, 512), BF16),
        scratch_shapes=[pltpu.SemaphoreType.DMA],
        compiler_params=SMALL,
        name="load",
    )(out_w)
    mixed = pl.pallas_call(
        output_kernel,
        in_specs=[pl.BlockSpec(memory_space=pltpu.VMEM)] * 4
        + [pl.BlockSpec(memory_space=pltpu.HBM)],
        out_shape=jax.ShapeDtypeStruct((64, 2048), BF16),
        scratch_shapes=[
            pltpu.VMEM((64, 1024), BF16), pltpu.VMEM((2048, 512), BF16), pltpu.SemaphoreType.DMA
        ],
        compiler_params=SMALL, name="output",
    )(near(mine), rec_gains, conv_gains, near(out_w0), out_w)
    return mixed[None]


def solution(mesh):
    finer = Mesh(
        mesh.devices.reshape(8, 8, mesh.shape["fs"], mesh.shape["tp"]), (Z, Y, X, C)
    )
    sp, sp_tp = (Z, Y), (Z, Y, C)
    row = P(sp, C)
    placed = (
        P(X, sp_tp, None), P(), row, row, row, row, P(None, C), P(X, None, C, sp), P(C),
        row, row, P(None, C), P(C), P(C, sp), P(C, sp),
    )
    return jax.shard_map(
        body, mesh=finer, in_specs=placed, out_specs=P(X, sp_tp, None), check_vma=False
    )
```

```python
import jax
import jax.numpy as jnp
from jax import lax
from jax.experimental import pallas as pl
from jax.experimental.pallas import tpu as pltpu
from jax.sharding import Mesh
from jax.sharding import PartitionSpec as P

KD = 128
BLOCK = 64
TILE = 256
SMALL = pltpu.CompilerParams(vmem_limit_bytes=24 * 1024 * 1024)
EPS = 1e-06
Z, Y, X, C = "sp_0", "sp_1", "fs", "tp"
F32, BF16 = jnp.float32, jnp.bfloat16
NN = (((1,), (0,)), ((), ()))
NT = (((1,), (1,)), ((), ()))
TN = (((0,), (0,)), ((), ()))


def dot(a, b, dims):
    return lax.dot_general(a, b, dims, preferred_element_type=F32)


def sigmoid(x):
    return 1.0 / (1.0 + jnp.exp(-x))


def lanes(rows):
    return lax.broadcasted_iota(jnp.int32, (rows, 128), 1)


def triangles():
    r = lax.broadcasted_iota(jnp.int32, (128, 128), 0)
    c = lax.broadcasted_iota(jnp.int32, (128, 128), 1)
    same = (r // BLOCK) == (c // BLOCK)
    return same & (c <= r), same & (c >= r)


def split_dot(mask, x):
    hi = x.astype(BF16)
    lo = (x - hi.astype(F32)).astype(BF16)
    return dot(mask, jnp.concatenate([hi, lo], axis=0), NN)


def project(x_ref, w_ref, rows, width):
    acc = jnp.zeros((rows.stop - rows.start, width), F32)
    for k in range(8):
        acc += dot(x_ref[rows, 256 * k : 256 * (k + 1)], w_ref[k], NT)
    return acc


def gate_product(acc):
    glu = acc.astype(BF16).astype(F32)
    return glu[:, 0:32] * sigmoid(glu[:, 32:64])


def gate_keys(a, gap):
    return gap * sigmoid(-a)


def start_kernel(
    x_ref, gain_ref, rf_ref, rb_ref, rq_ref, cv_ref, cg_ref, ri_ref, ld_ref, rec_ref, conv_ref,
    norm_ref, out_ref,
):
    for r in range(0, 64, 16):
        x = x_ref[r : r + 16, :].astype(F32)
        scale = lax.rsqrt(jnp.mean(x * x, axis=1, keepdims=True) + EPS)
        norm_ref[r : r + 16, :] = (x * scale * gain_ref[...]).astype(BF16)
    group = lanes(32) // 32
    row = lax.broadcasted_iota(jnp.int32, (32, 128), 0)
    for m in range(2):
        cols = slice(128 * m, 128 * (m + 1))
        src = [r[:, cols].astype(F32) for r in (rf_ref, rb_ref, rq_ref, cv_ref)]
        gate = cg_ref[:, cols].astype(F32)
        decays = jnp.zeros((32, 128), F32)
        for d in range(2):
            rest = jnp.broadcast_to(ld_ref[d, m : m + 1, :], (8, 128))
            for s in range(3):
                part = rest.astype(BF16).astype(F32)
                rest = rest - part
                low = pltpu.roll(part, 32, 1)[0:1]
                high = pltpu.roll(part, 64, 1)[0:1]
                decays = jnp.where(row == 2 * s + d, low, decays)
                decays = jnp.where(row == 6 + 2 * s + d, high, decays)
        for q in range(4):
            y = 4 * m + q
            a = jnp.zeros((32, 128), F32)
            for p in range(4):
                shift = (32 * (p - q)) % 128
                moved = pltpu.roll(src[p], shift, 1) if shift else src[p]
                a = jnp.where(group == p, moved, a)
            out_ref[y, :, 0:128] = a.astype(BF16)
            out_ref[y, :, 128:256] = ri_ref[:, cols]
            shift = (-32 * q) % 128
            moved = pltpu.roll(gate, shift, 1) if shift else gate
            out_ref[y, :, 256:384] = jnp.where(group == 0, moved, decays).astype(BF16)
            out_ref[y, :, 384:640] = rec_ref[...]
            out_ref[y, :, 640:896] = conv_ref[...]


def second_kernel(
    first_ref, gap_ref, taps_ref, w_ref, w2_ref, cols_ref, ld_ref, gap_out, taps_out
):
    gap_out[...] = gap_ref[...]
    taps_out[...] = taps_ref[...]
    lane = lanes(8)
    keys, values, gates = [], [], []
    for y in range(8):
        third = first_ref[y, :, 256:384].astype(F32)
        keys.append(first_ref[y, :, 0:128].astype(F32))
        values.append(first_ref[y, :, 128:256].astype(F32))
        gates.append(third)
        cols_ref[32 * y : 32 * (y + 1), :] = first_ref[y, :, 384:896]
        low = third[0:2] + third[2:4] + third[4:6]
        high = third[6:8] + third[8:10] + third[10:12]
        low = jnp.concatenate([low, low, low, low], axis=0)
        high = jnp.concatenate([high, high, high, high], axis=0)
        ld_ref[y] = jnp.where(lane < 96, pltpu.roll(low, 96, 1), pltpu.roll(high, 64, 1))[0:2]
    keys = jnp.concatenate(keys, axis=0).T.astype(BF16)
    w_ref[0:128, :] = jnp.concatenate(values, axis=0).T.astype(BF16)
    w_ref[128:224, :] = keys[0:96]
    gates = jnp.concatenate(gates, axis=0).T[0:32].astype(BF16)
    for i in range(8):
        w2_ref[i, 0:32, :] = keys[96:128]
        w2_ref[i, 32:64, :] = gates


def states_kernel(
    z_ref, x_hbm, w_ref, w2_ref, ld_ref, gap_ref,
    a_ref, v_ref, c_ref, send_ref, before_ref, offset_ref,
    x_ref, sems, chunk_s, chunk_t,
):
    z = z_ref[0]
    rows = TILE
    total = x_ref.shape[0]
    n = total // 64
    copies = []
    for t in range(total // rows):
        at = pl.ds(rows * t, rows)
        copies.append(pltpu.make_async_copy(x_hbm.at[at], x_ref.at[at], sems.at[t]))
        copies[-1].start()
    lower, upper = triangles()
    lower_f, upper_f = lower.astype(F32), upper.astype(F32)
    lower_b = lower_f.astype(BF16)
    lower_b = jnp.concatenate([lower_b, lower_b], axis=1)
    lane = lanes(128)
    lane1 = lanes(1)

    def gates(b):
        at = slice(128 * b, 128 * (b + 1))
        a = a_ref[at, :].astype(F32)
        v = v_ref[at, :]
        k = gate_keys(a, gap_ref[...])
        g = jnp.log1p(-k)
        ld = ld_ref[b]
        sums = split_dot(lower_b, g)
        first, second = sums[63:64], sums[127:128]
        ends = jnp.concatenate(
            [jnp.broadcast_to(first, (64, 128)), jnp.broadcast_to(second, (64, 128))], axis=0
        )
        cum_f = sums + jnp.sum(lower_f * ld[0:1], axis=1, keepdims=True)
        cum_b = ends - sums + g + jnp.sum(upper_f * ld[1:2], axis=1, keepdims=True)
        cum = jnp.where(lane < 32, cum_f, cum_b)
        c_ref[at, :] = cum
        for h in range(2):
            part = slice(64 * h, 64 * (h + 1))
            cc = cum[part]
            tot = jnp.where(lane1 < 32, cc[63:64], cc[0:1])
            kd = (k[part] * jnp.exp(tot - cc)).astype(BF16)
            st = dot(v[part], kd, TN)
            tot8 = jnp.broadcast_to(tot, (8, 128))
            tot8 = jnp.where(lanes(8) < 64, tot8, pltpu.roll(tot8, 64, 1))
            chunk_s[2 * b + h] = st[:64] + pltpu.roll(st[64:], 64, 1)
            chunk_t[2 * b + h] = tot8

    for t, copy in enumerate(copies):
        copy.wait()
        at = slice(rows * t, rows * (t + 1))
        acc = project(x_ref, w_ref, at, 224)
        if t:
            for b in range(rows // 128):
                gates((t - 1) * (rows // 128) + b)
        v_ref[at, :] = acc[:, :128].astype(BF16)
        a_ref[at, :] = jnp.concatenate([acc[:, 128:], jnp.zeros((rows, 32), F32)], axis=1).astype(BF16)
    head = gate_product(project(x_ref, w2_ref, slice(0, 16), 64))
    last = gate_product(project(x_ref, w2_ref, slice(total - 16, total), 64))
    for b in range(total // 128 - rows // 128, total // 128):
        gates(b)

    fwd = (lanes(64) % 64) < 32
    fwd8 = (lanes(8) % 64) < 32
    s = jnp.zeros((64, 128), F32)
    off = jnp.zeros((8, 128), F32)
    befores, offs = [None] * n, [None] * n
    for i in range(n):
        j = n - 1 - i
        befores[i], offs[i] = s, off
        tt = jnp.where(fwd8, chunk_t[i], chunk_t[j])
        sc = jnp.where(fwd, chunk_s[i], chunk_s[j])
        s = s * jnp.exp(tt)[0:1] + sc
        off = off + tt
        if i >= n // 2:
            for p, q in ((i, j), (j, i)):
                before_ref[p] = jnp.where(fwd, befores[p], befores[q]).astype(BF16)
                offset_ref[p] = jnp.where(fwd8, offs[p], offs[q])
    dec = jnp.exp(off)
    hi = dec.astype(BF16).astype(F32)
    lo = dec - hi
    fwd32 = (lanes(32) % 64) < 32
    later = jnp.where(fwd32, s[0:32], pltpu.roll(s[32:64], 32, 1))
    earlier = jnp.where(fwd32, pltpu.roll(s[0:32], 96, 1), s[32:64])
    row = lax.broadcasted_iota(jnp.int32, (16, 128), 0)
    edge = jnp.concatenate([head, last, last, last], axis=1)

    def with_decay(hi, lo):
        return jnp.where(lanes(16) < 64, edge, jnp.where(row == 0, hi[0:1], lo[0:1]))

    later_tail = with_decay(hi, lo)
    earlier_tail = with_decay(pltpu.roll(hi, 96, 1), pltpu.roll(lo, 96, 1))
    for i in range(8):
        ahead = jnp.where(i > z, 1, 0) > 0
        send_ref[i, 0:32, :] = jnp.where(ahead, later, earlier).astype(BF16)
        send_ref[i, 32:48, :] = jnp.where(ahead, later_tail, earlier_tail).astype(BF16)


def local_kernel(
    x_hbm, w2_ref, a_ref, v_ref, c_ref, gap_ref, before_ref, offset_ref, taps_ref,
    out_ref, qd_ref, conv_ref, edge_ref, x_ref, sems, pad,
):
    n = x_ref.shape[0]
    copies = []
    for t in range(n // TILE):
        at = pl.ds(TILE * t, TILE)
        copies.append(pltpu.make_async_copy(x_hbm.at[at], x_ref.at[at], sems.at[t]))
        copies[-1].start()
    lower, upper = triangles()
    lane = lanes(128)
    for b in range(a_ref.shape[0] // 128):
        rows = slice(128 * b, 128 * (b + 1))
        a = a_ref[rows, :].astype(F32)
        v = v_ref[rows, :]
        cum = c_ref[rows, :]
        k = gate_keys(a, gap_ref[...])
        q = a * sigmoid(a) * (KD ** -0.5)
        q = jnp.where(lane < 32, pltpu.roll(q, 64, 1), pltpu.roll(q, 96, 1))
        q = jnp.where(lane < 64, q, 0.0)
        qg = q * jnp.exp(cum)
        kn = (k * jnp.exp(-cum)).astype(BF16)
        qf = jnp.where(lane < 32, qg, 0.0).astype(BF16)
        qb = jnp.where(lane < 32, 0.0, qg).astype(BF16)
        qh = qg.astype(BF16)
        scores = jnp.where(lower, dot(qf, kn, NT), 0.0) + jnp.where(upper, dot(qb, kn, NT), 0.0)
        out = dot(scores.astype(BF16), v, NN)
        for h in range(2):
            part = slice(64 * h, 64 * (h + 1))
            to = slice(128 * b + 64 * h, 128 * b + 64 * (h + 1))
            sb = before_ref[2 * b + h]
            full = jnp.concatenate([sb, pltpu.roll(sb.astype(F32), 64, 1).astype(BF16)], axis=0)
            out_ref[to, :] = out[part] + dot(qh[part], full, NT)
            qd_ref[to, :] = (qg[part] * jnp.exp(offset_ref[2 * b + h][0:1])).astype(BF16)
    zeros = jnp.zeros((16, 32), F32)
    pad[0:16, :] = zeros
    for t, copy in enumerate(copies):
        copy.wait()
        acc = project(x_ref, w2_ref, slice(TILE * t, TILE * (t + 1)), 64)
        pad[16 + TILE * t : 16 + TILE * (t + 1), :] = gate_product(acc).astype(BF16).astype(F32)
    pad[16 + n : 32 + n, :] = zeros
    taps = taps_ref[...]
    for blk in range(n // 64):
        acc = jnp.zeros((64, 32), F32)
        for j in range(31):
            acc += pad[64 * blk + j + 1 : 64 * blk + j + 65, :] * taps[j : j + 1, :]
        conv_ref[blk] = jnp.concatenate([acc[16 * q : 16 * (q + 1)] for q in range(4)], axis=1).astype(BF16)
        if blk == 0:
            edge_ref[0] = acc[0:16]
        if blk == n // 64 - 1:
            edge_ref[1] = acc[48:64]


def merge_kernel(z_ref, recv_ref, local_ref, qd_ref, conv_ref, edge_ref, taps_ref, send_ref):
    z = z_ref[0]
    heads = jnp.zeros((16, 128), F32)
    tails = jnp.zeros((16, 128), F32)
    for i in range(8):
        other = recv_ref[i, 32:48, :].astype(F32)
        tails = jnp.where(i == z - 1, other, tails)
        heads = jnp.where(i == z + 1, other, heads)
    zeros = jnp.zeros((16, 32), F32)
    before = jnp.concatenate([tails[:, 32:64], zeros], axis=0)
    after = jnp.concatenate([zeros, heads[:, 0:32]], axis=0)
    first, last = edge_ref[0], edge_ref[1]
    taps = taps_ref[...]
    for j in range(15):
        first += before[j + 1 : j + 17] * taps[j : j + 1, :]
        last += after[j + 1 : j + 17] * taps[16 + j : 17 + j, :]
    first = jnp.concatenate([first] * 4, axis=1).astype(BF16)
    last = jnp.concatenate([last] * 4, axis=1).astype(BF16)
    lane16 = lanes(16)
    fwd = (lanes(64) % 64) < 32
    fwd1 = (lanes(1) % 64) < 32
    states, decays = [], []
    for i in range(8):
        packed = recv_ref[i, 0:32, :].astype(F32)
        states.append((packed, pltpu.roll(packed, 96, 1), pltpu.roll(packed, 32, 1)))
        parts = recv_ref[i, 32:48, :].astype(F32)
        both = parts[0:8] + jnp.concatenate([parts[1:8], parts[0:1]], axis=0)
        both = jnp.where(lanes(8) < 64, pltpu.roll(both, 64, 1), both)
        decays.append((both[0:1], pltpu.roll(both, 32, 1)[0:1]))
    s = jnp.zeros((64, 128), F32)
    for i in range(8):
        j = 7 - i
        sc_f = jnp.concatenate([states[i][0], states[i][1]], axis=0)
        sc_b = jnp.concatenate([states[j][2], states[j][0]], axis=0)
        sc = jnp.where(fwd, sc_f, sc_b)
        dec = jnp.where(fwd1, decays[i][0], decays[j][1])
        pass_f = jnp.where(i < z, 1, 0)
        pass_b = jnp.where(j > z, 1, 0)
        passed = jnp.where(fwd, pass_f, pass_b) > 0
        s = jnp.where(passed, s * dec + sc, s)
    full = jnp.concatenate([s, pltpu.roll(s, 64, 1)], axis=0).astype(BF16)
    for blk in range(16):
        rows = slice(64 * blk, 64 * (blk + 1))
        out = local_ref[rows, :] + dot(qd_ref[rows, :], full, NT)
        send_ref[blk, :64, :] = out.astype(BF16)
        packed = conv_ref[blk]
        if blk == 0:
            packed = jnp.where(lane16 < 32, first, packed)
        if blk == 15:
            packed = jnp.where(lane16 >= 96, last, packed)
        send_ref[blk, 64:, :] = packed


def output_kernel(
    recv_ref, rec_gain_ref, conv_gain_ref, w0_ref, w_hbm, out_ref, act, w1_ref, sem
):
    copy = pltpu.make_async_copy(w_hbm.at[1], w1_ref, sem)
    copy.start()
    for c in range(2):
        for h in range(2):
            rec = sum(recv_ref[(4 * h + q) * 2 + c, :64, :].astype(F32) for q in range(4))
            rec = rec * lax.rsqrt(jnp.mean(rec * rec, axis=1, keepdims=True) + EPS)
            rec = rec * rec_gain_ref[2 * c + h : 2 * c + h + 1, :]
            at = 128 * (4 * c + h)
            act[:, at : at + 128] = rec.astype(BF16)
    lane = lanes(16) // 32
    blocks = []
    for c in range(2):
        for m in range(2):
            parts = [recv_ref[(4 * m + q) * 2 + c, 64:80, :].astype(F32) for q in range(4)]
            groups = []
            for g in range(4):
                value = jnp.zeros((16, 128), F32)
                for q in range(4):
                    moved = parts[q] if q == g else pltpu.roll(parts[q], (32 * (q - g)) % 128, 1)
                    value = jnp.where(lane == q, moved, value)
                groups.append(value)
            blocks.append(jnp.concatenate(groups, axis=0))
    total = sum(jnp.sum(b, axis=1, keepdims=True) for b in blocks)
    square = sum(jnp.sum(b * b, axis=1, keepdims=True) for b in blocks)
    mean = total / 512.0
    scale = lax.rsqrt(square / 512.0 - mean * mean + EPS)
    for c in range(2):
        for m in range(2):
            n = 2 * c + m
            y = (blocks[n] - mean) * scale * conv_gain_ref[n : n + 1, :]
            at = 128 * (4 * c + 2 + m)
            act[:, at : at + 128] = (y * sigmoid(y)).astype(BF16)

    half = dot(act[:, 0:512], w0_ref[...], NT)
    copy.wait()
    out_ref[...] = (half + dot(act[:, 512:1024], w1_ref[...], NT)).astype(BF16)


def load_kernel(w_hbm, w_ref, sem):
    copy = pltpu.make_async_copy(w_hbm.at[0], w_ref, sem)
    copy.start()
    copy.wait()


def near(x):
    return pltpu.with_memory_space_constraint(x, pltpu.VMEM)


def kept(shape, dtype):
    return pltpu.VMEM(shape, dtype)


def body(
    tokens, norm_gain, rec_query, rec_input, rec_forward, rec_backward, forget_gap, log_decay,
    rec_gain, conv_value, conv_gate, conv_kernel, conv_gain, out_rec, out_conv,
):
    y, z = lax.axis_index(Y), lax.axis_index(Z)

    gap = lax.dynamic_index_in_dim(forget_gap.reshape(2, 8, 32), y, 1, keepdims=False)
    gap = jnp.pad(gap.reshape(1, 64), ((0, 0), (0, 64)))
    taps = lax.dynamic_index_in_dim(conv_kernel.reshape(31, 8, 32), y, 1, keepdims=False)
    taps = jnp.pad(taps.astype(F32), ((0, 1), (0, 0)))
    normed, first = pl.pallas_call(
        start_kernel,
        out_shape=[kept((64, 2048), BF16), kept((8, 32, 896), BF16)],
        name="start",
    )(
        tokens[0], norm_gain.reshape(1, 2048), rec_forward, rec_backward, rec_query, conv_value,
        conv_gate, rec_input, log_decay[0], out_rec.T, out_conv.T,
    )
    seq = lax.all_gather(normed, (Y, C), axis=0, tiled=True)
    first = lax.all_to_all(first, Y, split_axis=0, concat_axis=0, tiled=True)
    second, second2, out_cols, decays, gap, taps = pl.pallas_call(
        second_kernel,
        out_shape=[
            kept((224, 256), BF16),
            kept((8, 64, 256), BF16),
            jax.ShapeDtypeStruct((256, 512), BF16),
            kept((8, 2, 128), F32),
            kept((1, 128), F32),
            kept((32, 32), F32),
        ],
        name="second",
    )(near(first), near(gap), near(taps))
    weights2 = lax.all_to_all(second2, Z, split_axis=0, concat_axis=0, tiled=True)
    weights = lax.all_gather(second, Z, axis=0)
    out_w = lax.all_gather(out_cols, (C, Z), axis=0, tiled=True).reshape(2, 2048, 512)

    gains = lax.all_gather(jnp.stack([rec_gain, conv_gain]), C)
    rec_gains = gains[:, 0].reshape(4, 128)
    conv_gains = gains[:, 1].reshape(4, 128)
    n = seq.shape[0]
    seq = pltpu.with_memory_space_constraint(seq, pltpu.HBM)
    weights2 = near(weights2)
    z = z.reshape(1).astype(jnp.int32)
    pre_a, pre_v, cum, sent, before, offset = pl.pallas_call(
        states_kernel,
        in_specs=[pl.BlockSpec(memory_space=pltpu.SMEM), pl.BlockSpec(memory_space=pltpu.HBM)]
        + [pl.BlockSpec(memory_space=pltpu.VMEM)] * 4,
        out_shape=[
            kept((n, 128), BF16),
            kept((n, 128), BF16),
            kept((n, 128), F32),
            kept((8, 48, 128), BF16),
            kept((16, 64, 128), BF16),
            kept((16, 8, 128), F32),
        ],
        scratch_shapes=[
            pltpu.VMEM((n, 2048), BF16), pltpu.SemaphoreType.DMA((n // TILE,)),
            pltpu.VMEM((16, 64, 128), F32), pltpu.VMEM((16, 8, 128), F32),
        ],
        compiler_params=SMALL, name="states",
    )(z, seq, near(weights), weights2, near(decays), near(gap))

    arrived = lax.all_to_all(sent, Z, split_axis=0, concat_axis=0, tiled=True)
    local, decayed, convolved, edges = pl.pallas_call(
        local_kernel,
        out_shape=[
            kept((n, 128), F32),
            kept((n, 128), BF16),
            kept((16, 16, 128), BF16),
            kept((2, 16, 32), F32),
        ],
        in_specs=[pl.BlockSpec(memory_space=pltpu.HBM)]
        + [pl.BlockSpec(memory_space=pltpu.VMEM)] * 8,
        scratch_shapes=[
            pltpu.VMEM((n, 2048), BF16), pltpu.SemaphoreType.DMA((n // TILE,)),
            pltpu.VMEM((n + 32, 32), F32),
        ],
        compiler_params=SMALL, name="local",
    )(
        seq, weights2, near(pre_a), near(pre_v), near(cum), near(gap), near(before), near(offset),
        near(taps),
    )
    merged = pl.pallas_call(
        merge_kernel,
        in_specs=[pl.BlockSpec(memory_space=pltpu.SMEM)]
        + [pl.BlockSpec(memory_space=pltpu.VMEM)] * 6,
        out_shape=kept((16, 80, 128), BF16),
        compiler_params=SMALL, name="merge",
    )(z, near(arrived), near(local), near(decayed), near(convolved), near(edges), near(taps))
    mine = lax.all_to_all(merged, (Y, C), split_axis=0, concat_axis=0, tiled=True)
    out_w = pltpu.with_memory_space_constraint(out_w, pltpu.HBM)
    out_w0 = pl.pallas_call(
        load_kernel,
        in_specs=[pl.BlockSpec(memory_space=pltpu.HBM)],
        out_shape=kept((2048, 512), BF16),
        scratch_shapes=[pltpu.SemaphoreType.DMA],
        compiler_params=SMALL,
        name="load",
    )(out_w)
    mixed = pl.pallas_call(
        output_kernel,
        in_specs=[pl.BlockSpec(memory_space=pltpu.VMEM)] * 4
        + [pl.BlockSpec(memory_space=pltpu.HBM)],
        out_shape=jax.ShapeDtypeStruct((64, 2048), BF16),
        scratch_shapes=[
            pltpu.VMEM((64, 1024), BF16), pltpu.VMEM((2048, 512), BF16), pltpu.SemaphoreType.DMA
        ],
        compiler_params=SMALL, name="output",
    )(near(mine), rec_gains, conv_gains, near(out_w0), out_w)
    return mixed[None]


def solution(mesh):
    finer = Mesh(
        mesh.devices.reshape(8, 8, mesh.shape["fs"], mesh.shape["tp"]), (Z, Y, X, C)
    )
    sp, sp_tp = (Z, Y), (Z, Y, C)
    row = P(sp, C)
    placed = (
        P(X, sp_tp, None), P(), row, row, row, row, P(None, C), P(X, None, C, sp), P(C),
        row, row, P(None, C), P(C), P(C, sp), P(C, sp),
    )
    return jax.shard_map(
        body, mesh=finer, in_specs=placed, out_specs=P(X, sp_tp, None), check_vma=False
    )
```

```python
import jax
import jax.numpy as jnp
from jax import lax
from jax.experimental import pallas as pl
from jax.experimental.pallas import tpu as pltpu
from jax.sharding import Mesh
from jax.sharding import PartitionSpec as P

KD = 128
BLOCK = 64
TILE = 512
SMALL = pltpu.CompilerParams(vmem_limit_bytes=24 * 1024 * 1024)
EPS = 1e-06
Z, Y, X, C = "sp_0", "sp_1", "fs", "tp"
F32, BF16 = jnp.float32, jnp.bfloat16
NN = (((1,), (0,)), ((), ()))
NT = (((1,), (1,)), ((), ()))
TN = (((0,), (0,)), ((), ()))


def dot(a, b, dims):
    return lax.dot_general(a, b, dims, preferred_element_type=F32)


def sigmoid(x):
    return 1.0 / (1.0 + jnp.exp(-x))


def lanes(rows):
    return lax.broadcasted_iota(jnp.int32, (rows, 128), 1)


def triangles():
    r = lax.broadcasted_iota(jnp.int32, (128, 128), 0)
    c = lax.broadcasted_iota(jnp.int32, (128, 128), 1)
    same = (r // BLOCK) == (c // BLOCK)
    return same & (c <= r), same & (c >= r)


def split_dot(mask, x):
    hi = x.astype(BF16)
    lo = (x - hi.astype(F32)).astype(BF16)
    return dot(mask, jnp.concatenate([hi, lo], axis=0), NN)


def project(x_ref, w_ref, rows, width):
    acc = jnp.zeros((rows.stop - rows.start, width), F32)
    for k in range(8):
        acc += dot(x_ref[rows, 256 * k : 256 * (k + 1)], w_ref[k], NT)
    return acc


def rounded(acc):
    return acc.astype(BF16).astype(F32)


def gate_keys(a, gap):
    return gap * sigmoid(-a)


def start_kernel(
    x_ref, gain_ref, rf_ref, rb_ref, rq_ref, cv_ref, cg_ref, ri_ref, ld_ref, rec_ref, conv_ref,
    norm_ref, out_ref,
):
    for r in range(0, 64, 16):
        x = x_ref[r : r + 16, :].astype(F32)
        scale = lax.rsqrt(jnp.mean(x * x, axis=1, keepdims=True) + EPS)
        norm_ref[r : r + 16, :] = (x * scale * gain_ref[...]).astype(BF16)
    group = lanes(32) // 32
    row = lax.broadcasted_iota(jnp.int32, (32, 128), 0)
    for m in range(2):
        cols = slice(128 * m, 128 * (m + 1))
        src = [r[:, cols].astype(F32) for r in (rf_ref, rb_ref, rq_ref, ri_ref)]
        value_c = cv_ref[:, cols].astype(F32)
        gate_c = cg_ref[:, cols].astype(F32)
        decays = jnp.zeros((32, 128), F32)
        for d in range(2):
            rest = jnp.broadcast_to(ld_ref[d, m : m + 1, :], (8, 128))
            for s in range(3):
                part = rest.astype(BF16).astype(F32)
                rest = rest - part
                low = pltpu.roll(part, 64, 1)[0:1]
                decays = jnp.where(row == 2 * s + d, low, decays)
                decays = jnp.where(row == 6 + 2 * s + d, part[0:1], decays)
        turned = [pltpu.roll(x, 64, 1) for x in src]
        for q in range(4):
            y = 4 * m + q
            keys, values = q // 2, q % 2
            fwd = turned[0] if keys else src[0]
            bwd = src[1] if keys else turned[1]
            query = turned[2] if keys else src[2]
            value = turned[3] if values else src[3]
            conv = pltpu.roll(value_c, (32 * (2 - q)) % 128, 1) if q != 2 else value_c
            gate = pltpu.roll(gate_c, (32 * (3 - q)) % 128, 1) if q != 3 else gate_c
            value = jnp.where(group < 2, value, jnp.where(group == 2, conv, gate))
            out_ref[y, :, 0:128] = jnp.where(group < 2, fwd, bwd).astype(BF16)
            out_ref[y, :, 128:256] = value.astype(BF16)
            out_ref[y, :, 256:384] = jnp.where(group < 2, query, decays).astype(BF16)
            out_ref[y, :, 384:640] = rec_ref[...]
            out_ref[y, :, 640:896] = conv_ref[...]


def second_kernel(
    first_ref, gap_ref, taps_ref, w_ref, w2_ref, cols_ref, ld_ref, gap_out, taps_out
):
    gap_out[...] = gap_ref[...]
    taps_out[...] = taps_ref[...]
    lane = lanes(8)
    tiles = [[], [], []]
    for y in range(8):
        for t in range(3):
            tiles[t].append(first_ref[y, :, 128 * t : 128 * (t + 1)].astype(F32))
        third = tiles[2][-1]
        cols_ref[32 * y : 32 * (y + 1), :] = first_ref[y, :, 384:896]
        low = third[0:2] + third[2:4] + third[4:6]
        high = third[6:8] + third[8:10] + third[10:12]
        low = jnp.concatenate([low, low, low, low], axis=0)
        high = jnp.concatenate([high, high, high, high], axis=0)
        ld_ref[y] = jnp.where(lane < 64, pltpu.roll(low, 64, 1), high)[0:2]
    keys, values, queries = [jnp.concatenate(t, axis=0).T.astype(BF16) for t in tiles]
    w_ref[0:128, :] = keys
    w_ref[128:224, :] = values[0:96]
    w_ref[224:248, :] = queries[0:24]
    for i in range(8):
        w2_ref[i, 0:32, :] = values[96:128]
        w2_ref[i, 32:72, :] = queries[24:64]


def states_kernel(
    z_ref, x_hbm, w_ref, w2_ref, ld_ref, gap_ref,
    a_ref, v_ref, c_ref, send_ref, before_ref, offset_ref,
    x_ref, sems, chunk_s, chunk_t,
):
    z = z_ref[0]
    rows = TILE
    total = x_ref.shape[0]
    n = total // 64
    copies = []
    for t in range(total // rows):
        at = pl.ds(rows * t, rows)
        copies.append(pltpu.make_async_copy(x_hbm.at[at], x_ref.at[at], sems.at[t]))
        copies[-1].start()
    lower, upper = triangles()
    lower_f, upper_f = lower.astype(F32), upper.astype(F32)
    lower_b = lower_f.astype(BF16)
    lower_b = jnp.concatenate([lower_b, lower_b], axis=1)
    lane = lanes(128)
    lane1 = lanes(1)

    def gates(b):
        at = slice(128 * b, 128 * (b + 1))
        a = a_ref[at, :].astype(F32)
        v = v_ref[at, 0:64]
        k = gate_keys(a, gap_ref[...])
        g = jnp.log1p(-k)
        ld = ld_ref[b]
        sums = split_dot(lower_b, g)
        first, second = sums[63:64], sums[127:128]
        ends = jnp.concatenate(
            [jnp.broadcast_to(first, (64, 128)), jnp.broadcast_to(second, (64, 128))], axis=0
        )
        cum_f = sums + jnp.sum(lower_f * ld[0:1], axis=1, keepdims=True)
        cum_b = ends - sums + g + jnp.sum(upper_f * ld[1:2], axis=1, keepdims=True)
        cum = jnp.where(lane < 64, cum_f, cum_b)
        c_ref[at, :] = cum
        for h in range(2):
            part = slice(64 * h, 64 * (h + 1))
            cc = cum[part]
            tot = jnp.where(lane1 < 64, cc[63:64], cc[0:1])
            kd = (k[part] * jnp.exp(tot - cc)).astype(BF16)
            chunk_s[2 * b + h] = dot(v[part], kd, TN)
            chunk_t[2 * b + h] = jnp.broadcast_to(tot, (8, 128))

    for t, copy in enumerate(copies):
        copy.wait()
        at = slice(rows * t, rows * (t + 1))
        acc = project(x_ref, w_ref, at, 248)
        if t:
            for b in range(rows // 128):
                gates((t - 1) * (rows // 128) + b)
        a_ref[at, :] = acc[:, :128].astype(BF16)
        v_ref[at, :] = jnp.concatenate([acc[:, 128:], jnp.zeros((rows, 8), F32)], axis=1).astype(BF16)
    ends = []
    for at in (slice(0, 16), slice(total - 16, total)):
        gate = rounded(project(x_ref, w2_ref, at, 72)[:, 0:32])
        ends.append(v_ref[at, :].astype(F32)[:, 64:96] * sigmoid(gate))
    head, last = ends
    for b in range(total // 128 - rows // 128, total // 128):
        gates(b)

    fwd = lanes(64) < 64
    fwd8 = lanes(8) < 64
    s = jnp.zeros((64, 128), F32)
    off = jnp.zeros((8, 128), F32)
    befores, offs = [None] * n, [None] * n
    for i in range(n):
        j = n - 1 - i
        befores[i], offs[i] = s, off
        tt = jnp.where(fwd8, chunk_t[i], chunk_t[j])
        sc = jnp.where(fwd, chunk_s[i], chunk_s[j])
        s = s * jnp.exp(tt)[0:1] + sc
        off = off + tt
        if i >= n // 2:
            for p, q in ((i, j), (j, i)):
                before_ref[p] = jnp.where(fwd, befores[p], befores[q]).astype(BF16)
                offset_ref[p] = jnp.where(fwd8, offs[p], offs[q])
    dec = jnp.exp(off)
    hi = dec.astype(BF16).astype(F32)
    lo = dec - hi
    fwd32 = lanes(32) < 64
    later = jnp.where(fwd32, s[0:32], pltpu.roll(s[32:64], 64, 1))
    earlier = jnp.where(fwd32, pltpu.roll(s[0:32], 64, 1), s[32:64])
    row = lax.broadcasted_iota(jnp.int32, (16, 128), 0)
    edge = jnp.concatenate([head, last, last, last], axis=1)

    def with_decay(hi, lo):
        return jnp.where(lanes(16) < 64, edge, jnp.where(row == 0, hi[0:1], lo[0:1]))

    later_tail = with_decay(pltpu.roll(hi, 64, 1), pltpu.roll(lo, 64, 1))
    earlier_tail = with_decay(hi, lo)
    for i in range(8):
        ahead = jnp.where(i > z, 1, 0) > 0
        send_ref[i, 0:32, :] = jnp.where(ahead, later, earlier).astype(BF16)
        send_ref[i, 32:48, :] = jnp.where(ahead, later_tail, earlier_tail).astype(BF16)


def local_kernel(
    x_hbm, w2_ref, a_ref, v_ref, c_ref, gap_ref, before_ref, offset_ref, taps_ref,
    out_ref, qd_ref, conv_ref, edge_ref, x_ref, sems, pad,
):
    n = x_ref.shape[0]
    copies = []
    for t in range(n // TILE):
        at = pl.ds(TILE * t, TILE)
        copies.append(pltpu.make_async_copy(x_hbm.at[at], x_ref.at[at], sems.at[t]))
        copies[-1].start()
    lower, upper = triangles()
    lane = lanes(128)
    zeros = jnp.zeros((16, 32), F32)
    pad[0:16, :] = zeros
    for b in range(n // 128):
        rows = slice(128 * b, 128 * (b + 1))
        if b % (TILE // 128) == 0:
            t = b // (TILE // 128)
            copies[t].wait()
            late = rounded(project(x_ref, w2_ref, slice(TILE * t, TILE * (t + 1)), 72))
        extra = late[128 * b - TILE * t : 128 * (b + 1) - TILE * t]
        mixed = v_ref[rows, :].astype(F32)
        v = v_ref[rows, 0:64]
        gated = mixed[:, 64:96] * sigmoid(extra[:, 0:32])
        pad[16 + 128 * b : 16 + 128 * (b + 1), :] = rounded(gated)
        a = a_ref[rows, :].astype(F32)
        cum = c_ref[rows, :]
        k = gate_keys(a, gap_ref[...])
        q = [mixed[:, 96:120], extra[:, 32:72]]
        q = jnp.concatenate(q + q, axis=1)
        q = q * sigmoid(q) * (KD ** -0.5)
        qg = q * jnp.exp(cum)
        kn = (k * jnp.exp(-cum)).astype(BF16)
        qf = jnp.where(lane < 64, qg, 0.0).astype(BF16)
        qb = jnp.where(lane < 64, 0.0, qg).astype(BF16)
        qh = qg.astype(BF16)
        scores = jnp.where(lower, dot(qf, kn, NT), 0.0) + jnp.where(upper, dot(qb, kn, NT), 0.0)
        out = dot(scores.astype(BF16), v, NN)
        for h in range(2):
            part = slice(64 * h, 64 * (h + 1))
            to = slice(128 * b + 64 * h, 128 * b + 64 * (h + 1))
            out_ref[to, :] = out[part] + dot(qh[part], before_ref[2 * b + h], NT)
            qd_ref[to, :] = (qg[part] * jnp.exp(offset_ref[2 * b + h][0:1])).astype(BF16)
    pad[16 + n : 32 + n, :] = zeros
    taps = taps_ref[...]
    for blk in range(n // 64):
        acc = jnp.zeros((64, 32), F32)
        for j in range(31):
            acc += pad[64 * blk + j + 1 : 64 * blk + j + 65, :] * taps[j : j + 1, :]
        conv_ref[blk] = jnp.concatenate([acc[16 * q : 16 * (q + 1)] for q in range(4)], axis=1).astype(BF16)
        if blk == 0:
            edge_ref[0] = acc[0:16]
        if blk == n // 64 - 1:
            edge_ref[1] = acc[48:64]


def merge_kernel(z_ref, recv_ref, local_ref, qd_ref, conv_ref, edge_ref, taps_ref, send_ref):
    z = z_ref[0]
    heads = jnp.zeros((16, 128), F32)
    tails = jnp.zeros((16, 128), F32)
    for i in range(8):
        other = recv_ref[i, 32:48, :].astype(F32)
        tails = jnp.where(i == z - 1, other, tails)
        heads = jnp.where(i == z + 1, other, heads)
    zeros = jnp.zeros((16, 32), F32)
    before = jnp.concatenate([tails[:, 32:64], zeros], axis=0)
    after = jnp.concatenate([zeros, heads[:, 0:32]], axis=0)
    first, last = edge_ref[0], edge_ref[1]
    taps = taps_ref[...]
    for j in range(15):
        first += before[j + 1 : j + 17] * taps[j : j + 1, :]
        last += after[j + 1 : j + 17] * taps[16 + j : 17 + j, :]
    first = jnp.concatenate([first] * 4, axis=1).astype(BF16)
    last = jnp.concatenate([last] * 4, axis=1).astype(BF16)
    lane16 = lanes(16)
    fwd = lanes(64) < 64
    fwd1 = lanes(1) < 64
    states, decays = [], []
    for i in range(8):
        packed = recv_ref[i, 0:32, :].astype(F32)
        states.append((packed, pltpu.roll(packed, 64, 1)))
        parts = recv_ref[i, 32:48, :].astype(F32)
        both = parts[0:8] + jnp.concatenate([parts[1:8], parts[0:1]], axis=0)
        decays.append((pltpu.roll(both, 64, 1)[0:1], both[0:1]))
    s = jnp.zeros((64, 128), F32)
    for i in range(8):
        j = 7 - i
        sc_f = jnp.concatenate([states[i][0], states[i][1]], axis=0)
        sc_b = jnp.concatenate([states[j][1], states[j][0]], axis=0)
        sc = jnp.where(fwd, sc_f, sc_b)
        dec = jnp.where(fwd1, decays[i][0], decays[j][1])
        pass_f = jnp.where(i < z, 1, 0)
        pass_b = jnp.where(j > z, 1, 0)
        passed = jnp.where(fwd, pass_f, pass_b) > 0
        s = jnp.where(passed, s * dec + sc, s)
    full = s.astype(BF16)
    for blk in range(16):
        rows = slice(64 * blk, 64 * (blk + 1))
        out = local_ref[rows, :] + dot(qd_ref[rows, :], full, NT)
        send_ref[blk, :32, :] = jnp.concatenate([out[0:32], out[32:64]], axis=1).astype(BF16)
        packed = conv_ref[blk]
        if blk == 0:
            packed = jnp.where(lane16 < 32, first, packed)
        if blk == 15:
            packed = jnp.where(lane16 >= 96, last, packed)
        send_ref[blk, 32:, :] = packed


def output_kernel(
    recv_ref, rec_gain_ref, conv_gain_ref, w0_ref, w_hbm, out_ref, act, w1_ref, sem
):
    copy = pltpu.make_async_copy(w_hbm.at[1], w1_ref, sem)
    copy.start()
    for c in range(2):
        for h in range(2):
            low, high = [
                recv_ref[(4 * h + v) * 2 + c, :32, :].astype(F32)
                + recv_ref[(4 * h + 2 + v) * 2 + c, :32, :].astype(F32)
                for v in range(2)
            ]
            left = lanes(32) < 64
            rec = jnp.concatenate(
                [
                    jnp.where(left, low, pltpu.roll(high, 64, 1)),
                    jnp.where(left, pltpu.roll(low, 64, 1), high),
                ],
                axis=0,
            )
            rec = rec * lax.rsqrt(jnp.mean(rec * rec, axis=1, keepdims=True) + EPS)
            rec = rec * rec_gain_ref[2 * c + h : 2 * c + h + 1, :]
            at = 128 * (4 * c + h)
            act[:, at : at + 128] = rec.astype(BF16)
    lane = lanes(16) // 32
    blocks = []
    for c in range(2):
        for m in range(2):
            parts = [recv_ref[(4 * m + q) * 2 + c, 32:48, :].astype(F32) for q in range(4)]
            groups = []
            for g in range(4):
                value = jnp.zeros((16, 128), F32)
                for q in range(4):
                    moved = parts[q] if q == g else pltpu.roll(parts[q], (32 * (q - g)) % 128, 1)
                    value = jnp.where(lane == q, moved, value)
                groups.append(value)
            blocks.append(jnp.concatenate(groups, axis=0))
    total = sum(jnp.sum(b, axis=1, keepdims=True) for b in blocks)
    square = sum(jnp.sum(b * b, axis=1, keepdims=True) for b in blocks)
    mean = total / 512.0
    scale = lax.rsqrt(square / 512.0 - mean * mean + EPS)
    for c in range(2):
        for m in range(2):
            n = 2 * c + m
            y = (blocks[n] - mean) * scale * conv_gain_ref[n : n + 1, :]
            at = 128 * (4 * c + 2 + m)
            act[:, at : at + 128] = (y * sigmoid(y)).astype(BF16)

    half = dot(act[:, 0:512], w0_ref[...], NT)
    copy.wait()
    out_ref[...] = (half + dot(act[:, 512:1024], w1_ref[...], NT)).astype(BF16)


def load_kernel(w_hbm, w_ref, sem):
    copy = pltpu.make_async_copy(w_hbm.at[0], w_ref, sem)
    copy.start()
    copy.wait()


def near(x):
    return pltpu.with_memory_space_constraint(x, pltpu.VMEM)


def kept(shape, dtype):
    return pltpu.VMEM(shape, dtype)


def body(
    tokens, norm_gain, rec_query, rec_input, rec_forward, rec_backward, forget_gap, log_decay,
    rec_gain, conv_value, conv_gate, conv_kernel, conv_gain, out_rec, out_conv,
):
    y, z = lax.axis_index(Y), lax.axis_index(Z)

    gap = lax.dynamic_index_in_dim(forget_gap.reshape(2, 4, 64), y // 2, 1, keepdims=False)
    gap = gap.reshape(1, 128)
    taps = lax.dynamic_index_in_dim(conv_kernel.reshape(31, 8, 32), y, 1, keepdims=False)
    taps = jnp.pad(taps.astype(F32), ((0, 1), (0, 0)))
    normed, first = pl.pallas_call(
        start_kernel,
        out_shape=[kept((64, 2048), BF16), kept((8, 32, 896), BF16)],
        name="start",
    )(
        tokens[0], norm_gain.reshape(1, 2048), rec_forward, rec_backward, rec_query, conv_value,
        conv_gate, rec_input, log_decay[0], out_rec.T, out_conv.T,
    )
    seq = lax.all_gather(normed, (Y, C), axis=0, tiled=True)
    first = lax.all_to_all(first, Y, split_axis=0, concat_axis=0, tiled=True)
    second, second2, out_cols, decays, gap, taps = pl.pallas_call(
        second_kernel,
        out_shape=[
            kept((248, 256), BF16),
            kept((8, 72, 256), BF16),
            jax.ShapeDtypeStruct((256, 512), BF16),
            kept((8, 2, 128), F32),
            kept((1, 128), F32),
            kept((32, 32), F32),
        ],
        name="second",
    )(near(first), near(gap), near(taps))
    weights2 = lax.all_to_all(second2, Z, split_axis=0, concat_axis=0, tiled=True)
    weights = lax.all_gather(second, Z, axis=0)
    out_w = lax.all_gather(out_cols, (C, Z), axis=0, tiled=True).reshape(2, 2048, 512)

    gains = lax.all_gather(jnp.stack([rec_gain, conv_gain]), C)
    rec_gains = gains[:, 0].reshape(4, 128)
    conv_gains = gains[:, 1].reshape(4, 128)
    n = seq.shape[0]
    seq = pltpu.with_memory_space_constraint(seq, pltpu.HBM)
    weights2 = near(weights2)
    z = z.reshape(1).astype(jnp.int32)
    pre_a, pre_v, cum, sent, before, offset = pl.pallas_call(
        states_kernel,
        in_specs=[pl.BlockSpec(memory_space=pltpu.SMEM), pl.BlockSpec(memory_space=pltpu.HBM)]
        + [pl.BlockSpec(memory_space=pltpu.VMEM)] * 4,
        out_shape=[
            kept((n, 128), BF16),
            kept((n, 128), BF16),
            kept((n, 128), F32),
            kept((8, 48, 128), BF16),
            kept((16, 64, 128), BF16),
            kept((16, 8, 128), F32),
        ],
        scratch_shapes=[
            pltpu.VMEM((n, 2048), BF16), pltpu.SemaphoreType.DMA((n // TILE,)),
            pltpu.VMEM((16, 64, 128), F32), pltpu.VMEM((16, 8, 128), F32),
        ],
        compiler_params=SMALL, name="states",
    )(z, seq, near(weights), weights2, near(decays), near(gap))

    arrived = lax.all_to_all(sent, Z, split_axis=0, concat_axis=0, tiled=True)
    local, decayed, convolved, edges = pl.pallas_call(
        local_kernel,
        out_shape=[
            kept((n, 64), F32),
            kept((n, 128), BF16),
            kept((16, 16, 128), BF16),
            kept((2, 16, 32), F32),
        ],
        in_specs=[pl.BlockSpec(memory_space=pltpu.HBM)]
        + [pl.BlockSpec(memory_space=pltpu.VMEM)] * 8,
        scratch_shapes=[
            pltpu.VMEM((n, 2048), BF16), pltpu.SemaphoreType.DMA((n // TILE,)),
            pltpu.VMEM((n + 32, 32), F32),
        ],
        compiler_params=SMALL, name="local",
    )(
        seq, weights2, near(pre_a), near(pre_v), near(cum), near(gap), near(before), near(offset),
        near(taps),
    )
    merged = pl.pallas_call(
        merge_kernel,
        in_specs=[pl.BlockSpec(memory_space=pltpu.SMEM)]
        + [pl.BlockSpec(memory_space=pltpu.VMEM)] * 6,
        out_shape=kept((16, 48, 128), BF16),
        compiler_params=SMALL, name="merge",
    )(z, near(arrived), near(local), near(decayed), near(convolved), near(edges), near(taps))
    mine = lax.all_to_all(merged, (Y, C), split_axis=0, concat_axis=0, tiled=True)
    out_w = pltpu.with_memory_space_constraint(out_w, pltpu.HBM)
    out_w0 = pl.pallas_call(
        load_kernel,
        in_specs=[pl.BlockSpec(memory_space=pltpu.HBM)],
        out_shape=kept((2048, 512), BF16),
        scratch_shapes=[pltpu.SemaphoreType.DMA],
        compiler_params=SMALL,
        name="load",
    )(out_w)
    mixed = pl.pallas_call(
        output_kernel,
        in_specs=[pl.BlockSpec(memory_space=pltpu.VMEM)] * 4
        + [pl.BlockSpec(memory_space=pltpu.HBM)],
        out_shape=jax.ShapeDtypeStruct((64, 2048), BF16),
        scratch_shapes=[
            pltpu.VMEM((64, 1024), BF16), pltpu.VMEM((2048, 512), BF16), pltpu.SemaphoreType.DMA
        ],
        compiler_params=SMALL, name="output",
    )(near(mine), rec_gains, conv_gains, near(out_w0), out_w)
    return mixed[None]


def solution(mesh):
    finer = Mesh(
        mesh.devices.reshape(8, 8, mesh.shape["fs"], mesh.shape["tp"]), (Z, Y, X, C)
    )
    sp, sp_tp = (Z, Y), (Z, Y, C)
    row = P(sp, C)
    placed = (
        P(X, sp_tp, None), P(), row, row, row, row, P(None, C), P(X, None, C, sp), P(C),
        row, row, P(None, C), P(C), P(C, sp), P(C, sp),
    )
    return jax.shard_map(
        body, mesh=finer, in_specs=placed, out_specs=P(X, sp_tp, None), check_vma=False
    )
```

```python
import jax
import jax.numpy as jnp
from jax import lax
from jax.experimental import pallas as pl
from jax.experimental.pallas import tpu as pltpu
from jax.sharding import Mesh
from jax.sharding import PartitionSpec as P

KD = 128
BLOCK = 64
TILE = 256
SMALL = pltpu.CompilerParams(vmem_limit_bytes=24 * 1024 * 1024)
EPS = 1e-06
Z, Y, X, C = "sp_0", "sp_1", "fs", "tp"
F32, BF16 = jnp.float32, jnp.bfloat16
NN = (((1,), (0,)), ((), ()))
NT = (((1,), (1,)), ((), ()))
TN = (((0,), (0,)), ((), ()))


def dot(a, b, dims):
    return lax.dot_general(a, b, dims, preferred_element_type=F32)


def sigmoid(x):
    return 1.0 / (1.0 + jnp.exp(-x))


def lanes(rows):
    return lax.broadcasted_iota(jnp.int32, (rows, 128), 1)


def triangles():
    r = lax.broadcasted_iota(jnp.int32, (128, 128), 0)
    c = lax.broadcasted_iota(jnp.int32, (128, 128), 1)
    same = (r // BLOCK) == (c // BLOCK)
    return same & (c <= r), same & (c >= r)


def split_dot(mask, x):
    hi = x.astype(BF16)
    lo = (x - hi.astype(F32)).astype(BF16)
    return dot(mask, jnp.concatenate([hi, lo], axis=0), NN)


def project(x_ref, w_ref, rows, width):
    acc = jnp.zeros((rows.stop - rows.start, width), F32)
    for k in range(8):
        acc += dot(x_ref[rows, 256 * k : 256 * (k + 1)], w_ref[k], NT)
    return acc


def rounded(acc):
    return acc.astype(BF16).astype(F32)


def gate_keys(a, gap):
    return gap * sigmoid(-a)


def start_kernel(
    x_ref, gain_ref, rf_ref, rb_ref, rq_ref, cv_ref, cg_ref, ri_ref, ld_ref, rec_ref, conv_ref,
    norm_ref, out_ref,
):
    for r in range(0, 64, 16):
        x = x_ref[r : r + 16, :].astype(F32)
        scale = lax.rsqrt(jnp.mean(x * x, axis=1, keepdims=True) + EPS)
        norm_ref[r : r + 16, :] = (x * scale * gain_ref[...]).astype(BF16)
    group = lanes(32) // 32
    row = lax.broadcasted_iota(jnp.int32, (32, 128), 0)
    for m in range(2):
        cols = slice(128 * m, 128 * (m + 1))
        src = [r[:, cols].astype(F32) for r in (rf_ref, rb_ref, rq_ref, ri_ref)]
        value_c = cv_ref[:, cols].astype(F32)
        gate_c = cg_ref[:, cols].astype(F32)
        decays = jnp.zeros((32, 128), F32)
        for d in range(2):
            rest = jnp.broadcast_to(ld_ref[d, m : m + 1, :], (8, 128))
            for s in range(3):
                part = rest.astype(BF16).astype(F32)
                rest = rest - part
                low = pltpu.roll(part, 64, 1)[0:1]
                decays = jnp.where(row == 2 * s + d, low, decays)
                decays = jnp.where(row == 6 + 2 * s + d, part[0:1], decays)
        turned = [pltpu.roll(x, 64, 1) for x in src]
        for q in range(4):
            y = 4 * m + q
            keys, values = q // 2, q % 2
            fwd = turned[0] if keys else src[0]
            bwd = src[1] if keys else turned[1]
            query = turned[2] if keys else src[2]
            value = turned[3] if values else src[3]
            conv = pltpu.roll(value_c, (32 * (2 - q)) % 128, 1) if q != 2 else value_c
            gate = pltpu.roll(gate_c, (32 * (3 - q)) % 128, 1) if q != 3 else gate_c
            value = jnp.where(group < 2, value, jnp.where(group == 2, conv, gate))
            out_ref[y, :, 0:128] = jnp.where(group < 2, fwd, bwd).astype(BF16)
            out_ref[y, :, 128:256] = value.astype(BF16)
            out_ref[y, :, 256:384] = jnp.where(group < 2, query, decays).astype(BF16)
            out_ref[y, :, 384:640] = rec_ref[...]
            out_ref[y, :, 640:896] = conv_ref[...]


def second_kernel(
    first_ref, gap_ref, taps_ref, w_ref, w2_ref, cols_ref, ld_ref, gap_out, taps_out
):
    gap_out[...] = gap_ref[...]
    taps_out[...] = taps_ref[...]
    lane = lanes(8)
    tiles = [[], [], []]
    for y in range(8):
        for t in range(3):
            tiles[t].append(first_ref[y, :, 128 * t : 128 * (t + 1)].astype(F32))
        third = tiles[2][-1]
        cols_ref[32 * y : 32 * (y + 1), :] = first_ref[y, :, 384:896]
        low = third[0:2] + third[2:4] + third[4:6]
        high = third[6:8] + third[8:10] + third[10:12]
        low = jnp.concatenate([low, low, low, low], axis=0)
        high = jnp.concatenate([high, high, high, high], axis=0)
        ld_ref[y] = jnp.where(lane < 64, pltpu.roll(low, 64, 1), high)[0:2]
    keys, values, queries = [jnp.concatenate(t, axis=0).T.astype(BF16) for t in tiles]
    w_ref[0:128, :] = keys
    w_ref[128:224, :] = values[0:96]
    w_ref[224:248, :] = queries[0:24]
    for i in range(8):
        w2_ref[i, 0:32, :] = values[96:128]
        w2_ref[i, 32:72, :] = queries[24:64]


def states_kernel(
    z_ref, x_hbm, w_ref, w2_ref, ld_ref, gap_ref,
    a_ref, v_ref, c_ref, send_ref, before_ref, offset_ref,
    x_ref, sems, chunk_s, chunk_t,
):
    z = z_ref[0]
    rows = TILE
    total = x_ref.shape[0]
    n = total // 64
    copies = []
    for t in range(total // rows):
        at = pl.ds(rows * t, rows)
        copies.append(pltpu.make_async_copy(x_hbm.at[at], x_ref.at[at], sems.at[t]))
        copies[-1].start()
    lower, upper = triangles()
    lower_f, upper_f = lower.astype(F32), upper.astype(F32)
    lower_b = lower_f.astype(BF16)
    lower_b = jnp.concatenate([lower_b, lower_b], axis=1)
    lane = lanes(128)
    lane1 = lanes(1)

    def gates(b):
        at = slice(128 * b, 128 * (b + 1))
        a = a_ref[at, :].astype(F32)
        v = v_ref[at, 0:64]
        k = gate_keys(a, gap_ref[...])
        g = jnp.log1p(-k)
        ld = ld_ref[b]
        sums = split_dot(lower_b, g)
        first, second = sums[63:64], sums[127:128]
        ends = jnp.concatenate(
            [jnp.broadcast_to(first, (64, 128)), jnp.broadcast_to(second, (64, 128))], axis=0
        )
        cum_f = sums + jnp.sum(lower_f * ld[0:1], axis=1, keepdims=True)
        cum_b = ends - sums + g + jnp.sum(upper_f * ld[1:2], axis=1, keepdims=True)
        cum = jnp.where(lane < 64, cum_f, cum_b)
        c_ref[at, :] = cum
        for h in range(2):
            part = slice(64 * h, 64 * (h + 1))
            cc = cum[part]
            tot = jnp.where(lane1 < 64, cc[63:64], cc[0:1])
            kd = (k[part] * jnp.exp(tot - cc)).astype(BF16)
            chunk_s[2 * b + h] = dot(v[part], kd, TN)
            chunk_t[2 * b + h] = jnp.broadcast_to(tot, (8, 128))

    for t, copy in enumerate(copies):
        copy.wait()
        at = slice(rows * t, rows * (t + 1))
        acc = project(x_ref, w_ref, at, 248)
        if t:
            for b in range(rows // 128):
                gates((t - 1) * (rows // 128) + b)
        a_ref[at, :] = acc[:, :128].astype(BF16)
        v_ref[at, :] = jnp.concatenate([acc[:, 128:], jnp.zeros((rows, 8), F32)], axis=1).astype(BF16)
    both = jnp.zeros((32, 32), F32)
    for k in range(8):
        cols = slice(256 * k, 256 * (k + 1))
        xk = jnp.concatenate([x_ref[0:16, cols], x_ref[total - 16 : total, cols]], axis=0)
        both += dot(xk, w2_ref[k, 0:32, :], NT)
    both = sigmoid(rounded(both))
    head = v_ref[0:16, :].astype(F32)[:, 64:96] * both[0:16]
    last = v_ref[total - 16 : total, :].astype(F32)[:, 64:96] * both[16:32]
    for b in range(total // 128 - rows // 128, total // 128):
        gates(b)

    fwd = lanes(64) < 64
    fwd8 = lanes(8) < 64
    s = jnp.zeros((64, 128), F32)
    off = jnp.zeros((8, 128), F32)
    befores, offs = [None] * n, [None] * n
    for i in range(n):
        j = n - 1 - i
        befores[i], offs[i] = s, off
        tt = jnp.where(fwd8, chunk_t[i], chunk_t[j])
        sc = jnp.where(fwd, chunk_s[i], chunk_s[j])
        s = s * jnp.exp(tt)[0:1] + sc
        off = off + tt
        if i >= n // 2:
            for p, q in ((i, j), (j, i)):
                before_ref[p] = jnp.where(fwd, befores[p], befores[q]).astype(BF16)
                offset_ref[p] = jnp.where(fwd8, offs[p], offs[q])
    dec = jnp.exp(off)
    hi = dec.astype(BF16).astype(F32)
    lo = dec - hi
    fwd32 = lanes(32) < 64
    later = jnp.where(fwd32, s[0:32], pltpu.roll(s[32:64], 64, 1))
    earlier = jnp.where(fwd32, pltpu.roll(s[0:32], 64, 1), s[32:64])
    row = lax.broadcasted_iota(jnp.int32, (16, 128), 0)
    edge = jnp.concatenate([head, last, last, last], axis=1)

    def with_decay(hi, lo):
        return jnp.where(lanes(16) < 64, edge, jnp.where(row == 0, hi[0:1], lo[0:1]))

    later_tail = with_decay(pltpu.roll(hi, 64, 1), pltpu.roll(lo, 64, 1))
    earlier_tail = with_decay(hi, lo)
    for i in range(8):
        ahead = jnp.where(i > z, 1, 0) > 0
        send_ref[i, 0:32, :] = jnp.where(ahead, later, earlier).astype(BF16)
        send_ref[i, 32:48, :] = jnp.where(ahead, later_tail, earlier_tail).astype(BF16)


def local_kernel(
    x_hbm, w2_ref, a_ref, v_ref, c_ref, gap_ref, before_ref, offset_ref, taps_ref,
    out_ref, qd_ref, conv_ref, edge_ref, x_ref, sems, pad,
):
    n = x_ref.shape[0]
    copies = []
    for t in range(n // TILE):
        at = pl.ds(TILE * t, TILE)
        copies.append(pltpu.make_async_copy(x_hbm.at[at], x_ref.at[at], sems.at[t]))
        copies[-1].start()
    lower, upper = triangles()
    lane = lanes(128)
    zeros = jnp.zeros((16, 32), F32)
    pad[0:16, :] = zeros
    for b in range(n // 128):
        rows = slice(128 * b, 128 * (b + 1))
        if b % (TILE // 128) == 0:
            t = b // (TILE // 128)
            copies[t].wait()
            late = rounded(project(x_ref, w2_ref, slice(TILE * t, TILE * (t + 1)), 72))
        extra = late[128 * b - TILE * t : 128 * (b + 1) - TILE * t]
        mixed = v_ref[rows, :].astype(F32)
        v = v_ref[rows, 0:64]
        gated = mixed[:, 64:96] * sigmoid(extra[:, 0:32])
        pad[16 + 128 * b : 16 + 128 * (b + 1), :] = rounded(gated)
        a = a_ref[rows, :].astype(F32)
        cum = c_ref[rows, :]
        k = gate_keys(a, gap_ref[...])
        q = [mixed[:, 96:120], extra[:, 32:72]]
        q = jnp.concatenate(q + q, axis=1)
        q = q * sigmoid(q) * (KD ** -0.5)
        qg = q * jnp.exp(cum)
        kn = (k * jnp.exp(-cum)).astype(BF16)
        qf = jnp.where(lane < 64, qg, 0.0).astype(BF16)
        qb = jnp.where(lane < 64, 0.0, qg).astype(BF16)
        qh = qg.astype(BF16)
        scores = jnp.where(lower, dot(qf, kn, NT), 0.0) + jnp.where(upper, dot(qb, kn, NT), 0.0)
        out = dot(scores.astype(BF16), v, NN)
        for h in range(2):
            part = slice(64 * h, 64 * (h + 1))
            to = slice(128 * b + 64 * h, 128 * b + 64 * (h + 1))
            out_ref[to, :] = out[part] + dot(qh[part], before_ref[2 * b + h], NT)
            qd_ref[to, :] = (qg[part] * jnp.exp(offset_ref[2 * b + h][0:1])).astype(BF16)
    pad[16 + n : 32 + n, :] = zeros
    taps = taps_ref[...]
    for blk in range(n // 64):
        acc = jnp.zeros((64, 32), F32)
        for j in range(31):
            acc += pad[64 * blk + j + 1 : 64 * blk + j + 65, :] * taps[j : j + 1, :]
        conv_ref[blk] = jnp.concatenate([acc[16 * q : 16 * (q + 1)] for q in range(4)], axis=1).astype(BF16)
        if blk == 0:
            edge_ref[0] = acc[0:16]
        if blk == n // 64 - 1:
            edge_ref[1] = acc[48:64]


def merge_kernel(z_ref, recv_ref, local_ref, qd_ref, conv_ref, edge_ref, taps_ref, send_ref):
    z = z_ref[0]
    heads = jnp.zeros((16, 128), F32)
    tails = jnp.zeros((16, 128), F32)
    for i in range(8):
        other = recv_ref[i, 32:48, :].astype(F32)
        tails = jnp.where(i == z - 1, other, tails)
        heads = jnp.where(i == z + 1, other, heads)
    zeros = jnp.zeros((16, 32), F32)
    before = jnp.concatenate([tails[:, 32:64], zeros], axis=0)
    after = jnp.concatenate([zeros, heads[:, 0:32]], axis=0)
    first, last = edge_ref[0], edge_ref[1]
    taps = taps_ref[...]
    for j in range(15):
        first += before[j + 1 : j + 17] * taps[j : j + 1, :]
        last += after[j + 1 : j + 17] * taps[16 + j : 17 + j, :]
    first = jnp.concatenate([first] * 4, axis=1).astype(BF16)
    last = jnp.concatenate([last] * 4, axis=1).astype(BF16)
    lane16 = lanes(16)
    fwd = lanes(64) < 64
    fwd1 = lanes(1) < 64
    states, decays = [], []
    for i in range(8):
        packed = recv_ref[i, 0:32, :].astype(F32)
        states.append((packed, pltpu.roll(packed, 64, 1)))
        parts = recv_ref[i, 32:48, :].astype(F32)
        both = parts[0:8] + jnp.concatenate([parts[1:8], parts[0:1]], axis=0)
        decays.append((pltpu.roll(both, 64, 1)[0:1], both[0:1]))
    s = jnp.zeros((64, 128), F32)
    for i in range(8):
        j = 7 - i
        sc_f = jnp.concatenate([states[i][0], states[i][1]], axis=0)
        sc_b = jnp.concatenate([states[j][1], states[j][0]], axis=0)
        sc = jnp.where(fwd, sc_f, sc_b)
        dec = jnp.where(fwd1, decays[i][0], decays[j][1])
        pass_f = jnp.where(i < z, 1, 0)
        pass_b = jnp.where(j > z, 1, 0)
        passed = jnp.where(fwd, pass_f, pass_b) > 0
        s = jnp.where(passed, s * dec + sc, s)
    full = s.astype(BF16)
    for blk in range(16):
        rows = slice(64 * blk, 64 * (blk + 1))
        out = local_ref[rows, :] + dot(qd_ref[rows, :], full, NT)
        send_ref[blk, :32, :] = jnp.concatenate([out[0:32], out[32:64]], axis=1).astype(BF16)
        packed = conv_ref[blk]
        if blk == 0:
            packed = jnp.where(lane16 < 32, first, packed)
        if blk == 15:
            packed = jnp.where(lane16 >= 96, last, packed)
        send_ref[blk, 32:, :] = packed


def output_kernel(
    recv_ref, rec_gain_ref, conv_gain_ref, w0_ref, w_hbm, out_ref, act, w1_ref, sem
):
    copy = pltpu.make_async_copy(w_hbm.at[1], w1_ref, sem)
    copy.start()
    for c in range(2):
        for h in range(2):
            low, high = [
                recv_ref[(4 * h + v) * 2 + c, :32, :].astype(F32)
                + recv_ref[(4 * h + 2 + v) * 2 + c, :32, :].astype(F32)
                for v in range(2)
            ]
            left = lanes(32) < 64
            rec = jnp.concatenate(
                [
                    jnp.where(left, low, pltpu.roll(high, 64, 1)),
                    jnp.where(left, pltpu.roll(low, 64, 1), high),
                ],
                axis=0,
            )
            rec = rec * lax.rsqrt(jnp.mean(rec * rec, axis=1, keepdims=True) + EPS)
            rec = rec * rec_gain_ref[2 * c + h : 2 * c + h + 1, :]
            at = 128 * (4 * c + h)
            act[:, at : at + 128] = rec.astype(BF16)
    lane = lanes(16) // 32
    blocks = []
    for c in range(2):
        for m in range(2):
            parts = [recv_ref[(4 * m + q) * 2 + c, 32:48, :].astype(F32) for q in range(4)]
            groups = []
            for g in range(4):
                value = jnp.zeros((16, 128), F32)
                for q in range(4):
                    moved = parts[q] if q == g else pltpu.roll(parts[q], (32 * (q - g)) % 128, 1)
                    value = jnp.where(lane == q, moved, value)
                groups.append(value)
            blocks.append(jnp.concatenate(groups, axis=0))
    total = sum(jnp.sum(b, axis=1, keepdims=True) for b in blocks)
    square = sum(jnp.sum(b * b, axis=1, keepdims=True) for b in blocks)
    mean = total / 512.0
    scale = lax.rsqrt(square / 512.0 - mean * mean + EPS)
    for c in range(2):
        for m in range(2):
            n = 2 * c + m
            y = (blocks[n] - mean) * scale * conv_gain_ref[n : n + 1, :]
            at = 128 * (4 * c + 2 + m)
            act[:, at : at + 128] = (y * sigmoid(y)).astype(BF16)

    half = dot(act[:, 0:512], w0_ref[...], NT)
    copy.wait()
    out_ref[...] = (half + dot(act[:, 512:1024], w1_ref[...], NT)).astype(BF16)


def load_kernel(w_hbm, w_ref, sem):
    copy = pltpu.make_async_copy(w_hbm.at[0], w_ref, sem)
    copy.start()
    copy.wait()


def near(x):
    return pltpu.with_memory_space_constraint(x, pltpu.VMEM)


def kept(shape, dtype):
    return pltpu.VMEM(shape, dtype)


def body(
    tokens, norm_gain, rec_query, rec_input, rec_forward, rec_backward, forget_gap, log_decay,
    rec_gain, conv_value, conv_gate, conv_kernel, conv_gain, out_rec, out_conv,
):
    y, z = lax.axis_index(Y), lax.axis_index(Z)

    gap = lax.dynamic_index_in_dim(forget_gap.reshape(2, 4, 64), y // 2, 1, keepdims=False)
    gap = gap.reshape(1, 128)
    taps = lax.dynamic_index_in_dim(conv_kernel.reshape(31, 8, 32), y, 1, keepdims=False)
    taps = jnp.pad(taps.astype(F32), ((0, 1), (0, 0)))
    normed, first = pl.pallas_call(
        start_kernel,
        out_shape=[kept((64, 2048), BF16), kept((8, 32, 896), BF16)],
        name="start",
    )(
        tokens[0], norm_gain.reshape(1, 2048), rec_forward, rec_backward, rec_query, conv_value,
        conv_gate, rec_input, log_decay[0], out_rec.T, out_conv.T,
    )
    seq = lax.all_gather(normed, (Y, C), axis=0, tiled=True)
    first = lax.all_to_all(first, Y, split_axis=0, concat_axis=0, tiled=True)
    second, second2, out_cols, decays, gap, taps = pl.pallas_call(
        second_kernel,
        out_shape=[
            kept((248, 256), BF16),
            kept((8, 72, 256), BF16),
            jax.ShapeDtypeStruct((256, 512), BF16),
            kept((8, 2, 128), F32),
            kept((1, 128), F32),
            kept((32, 32), F32),
        ],
        name="second",
    )(near(first), near(gap), near(taps))
    weights2 = lax.all_to_all(second2, Z, split_axis=0, concat_axis=0, tiled=True)
    weights = lax.all_gather(second, Z, axis=0)
    out_w = lax.all_gather(out_cols, (C, Z), axis=0, tiled=True).reshape(2, 2048, 512)

    gains = lax.all_gather(jnp.stack([rec_gain, conv_gain]), C)
    rec_gains = gains[:, 0].reshape(4, 128)
    conv_gains = gains[:, 1].reshape(4, 128)
    n = seq.shape[0]
    seq = pltpu.with_memory_space_constraint(seq, pltpu.HBM)
    weights2 = near(weights2)
    z = z.reshape(1).astype(jnp.int32)
    pre_a, pre_v, cum, sent, before, offset = pl.pallas_call(
        states_kernel,
        in_specs=[pl.BlockSpec(memory_space=pltpu.SMEM), pl.BlockSpec(memory_space=pltpu.HBM)]
        + [pl.BlockSpec(memory_space=pltpu.VMEM)] * 4,
        out_shape=[
            kept((n, 128), BF16),
            kept((n, 128), BF16),
            kept((n, 128), F32),
            kept((8, 48, 128), BF16),
            kept((16, 64, 128), BF16),
            kept((16, 8, 128), F32),
        ],
        scratch_shapes=[
            pltpu.VMEM((n, 2048), BF16), pltpu.SemaphoreType.DMA((n // TILE,)),
            pltpu.VMEM((16, 64, 128), F32), pltpu.VMEM((16, 8, 128), F32),
        ],
        compiler_params=SMALL, name="states",
    )(z, seq, near(weights), weights2, near(decays), near(gap))

    arrived = lax.all_to_all(sent, Z, split_axis=0, concat_axis=0, tiled=True)
    local, decayed, convolved, edges = pl.pallas_call(
        local_kernel,
        out_shape=[
            kept((n, 64), F32),
            kept((n, 128), BF16),
            kept((16, 16, 128), BF16),
            kept((2, 16, 32), F32),
        ],
        in_specs=[pl.BlockSpec(memory_space=pltpu.HBM)]
        + [pl.BlockSpec(memory_space=pltpu.VMEM)] * 8,
        scratch_shapes=[
            pltpu.VMEM((n, 2048), BF16), pltpu.SemaphoreType.DMA((n // TILE,)),
            pltpu.VMEM((n + 32, 32), F32),
        ],
        compiler_params=SMALL, name="local",
    )(
        seq, weights2, near(pre_a), near(pre_v), near(cum), near(gap), near(before), near(offset),
        near(taps),
    )
    merged = pl.pallas_call(
        merge_kernel,
        in_specs=[pl.BlockSpec(memory_space=pltpu.SMEM)]
        + [pl.BlockSpec(memory_space=pltpu.VMEM)] * 6,
        out_shape=kept((16, 48, 128), BF16),
        compiler_params=SMALL, name="merge",
    )(z, near(arrived), near(local), near(decayed), near(convolved), near(edges), near(taps))
    mine = lax.all_to_all(merged, (Y, C), split_axis=0, concat_axis=0, tiled=True)
    out_w = pltpu.with_memory_space_constraint(out_w, pltpu.HBM)
    out_w0 = pl.pallas_call(
        load_kernel,
        in_specs=[pl.BlockSpec(memory_space=pltpu.HBM)],
        out_shape=kept((2048, 512), BF16),
        scratch_shapes=[pltpu.SemaphoreType.DMA],
        compiler_params=SMALL,
        name="load",
    )(out_w)
    mixed = pl.pallas_call(
        output_kernel,
        in_specs=[pl.BlockSpec(memory_space=pltpu.VMEM)] * 4
        + [pl.BlockSpec(memory_space=pltpu.HBM)],
        out_shape=jax.ShapeDtypeStruct((64, 2048), BF16),
        scratch_shapes=[
            pltpu.VMEM((64, 1024), BF16), pltpu.VMEM((2048, 512), BF16), pltpu.SemaphoreType.DMA
        ],
        compiler_params=SMALL, name="output",
    )(near(mine), rec_gains, conv_gains, near(out_w0), out_w)
    return mixed[None]


def solution(mesh):
    finer = Mesh(
        mesh.devices.reshape(8, 8, mesh.shape["fs"], mesh.shape["tp"]), (Z, Y, X, C)
    )
    sp, sp_tp = (Z, Y), (Z, Y, C)
    row = P(sp, C)
    placed = (
        P(X, sp_tp, None), P(), row, row, row, row, P(None, C), P(X, None, C, sp), P(C),
        row, row, P(None, C), P(C), P(C, sp), P(C, sp),
    )
    return jax.shard_map(
        body, mesh=finer, in_specs=placed, out_specs=P(X, sp_tp, None), check_vma=False
    )
```
